512 devices in a mesh: grp: 2 (over y), ep: 64 (over z, core), tp: 4 (over x).
Axes of the slice: x: 4, y: 2, z: 32, core: 2. Of those that a mesh axis runs over, the one named last changes fastest.
The devices are a block of a 4x8x32 slice.
Arguments:
- tokens: bfloat16 [24576, 2048], P(('grp', 'ep')), parts along dimension 0, may hold values from -6 to 6
- norm_gain: float32 [2048], replicated, may hold values from 0.1 to 1.9
- w_gate: bfloat16 [64, 2048, 1024], P('ep', None, 'tp'), may hold values from -0.3125 to 0.3125
- w_up: bfloat16 [64, 2048, 1024], P('ep', None, 'tp'), may hold values from -0.3125 to 0.3125
- w_down: bfloat16 [64, 1024, 2048], P('ep', 'tp'), may hold values from -0.09375 to 0.09375
- expert_ids: int32 [24576, 4], P(('grp', 'ep')), parts along dimension 0, may hold values from 0 to 63, all different within a row; in each aligned block of 192 rows (0 to 191, 192 to 383, ...) at most 16 rows name the same one
- gate_weights: float32 [24576, 4], P(('grp', 'ep')), parts along dimension 0, may hold values from 0.1 to 1
Outputs:
- mixed: bfloat16 [24576, 2048], P(('grp', 'ep'), 'tp'), parts along dimension 0
The draws below stay inside these ranges and needn't reach their ends.
There are 2 independent parts, one for each index of `grp`. The reference program is written for one: setup_inputs(seed, part) draws one part's arguments, and reference() takes and returns one part's arrays. A program takes and returns all parts, laid end to end along the dimension named above; an argument that names none is the same for every part. Nothing has to cross between parts.
Inputs may be any that keep to these rules, and one draw needn't show every extreme that they name: `expert_ids`: each row names 4 different experts; among the rows of one index of ep, no expert is named by more than 16 rows, a bound that some block reaches.
All inputs are finite; a program needn't handle non-finite values.
Results may differ from the reference program's by a relative error of at most 0.012.
Values may be sent and summed in bfloat16 or wider, within the bound.
A program may use at most 64 MiB of HBM per device.

```python
import math
import jax
import jax.numpy as jnp
import numpy as np
from jax import lax

D = 2048
FF = 1024
TOP_K = 4
TOK_DEV = 192
EXPERTS = 64
CAP = 16
TOKENS = 12288
N_EP = 64
N_TP = 4


def shard_levels(own_key, shape, cuts, least, largest):
    def one(dim, parts):
        steps = jax.random.uniform(jax.random.fold_in(jax.random.fold_in(own_key, 6), dim), (parts,), jnp.float32, least / len(cuts), largest / len(cuts))
        return jnp.repeat(jnp.exp(steps), shape[dim] // parts).reshape((-1,) + (1,) * (len(shape) - dim - 1))

    factor_of = one(*cuts[0])
    for cut in cuts[1:]:
        factor_of = factor_of * one(*cut)
    return factor_of


def deal_out(own_key, own, number, rows, count, top, most, skew):
    order = jax.random.permutation(own_key, count)
    heavy_load, ordinary = portions_of(count, rows * top, most, skew, True), portions_of(count, rows * top, most, skew, False)
    places = jnp.arange(count)

    def named(lengths, offset_by):
        used = int((lengths > 0).sum())
        fixed = max(1, used // 4)
        moved = fixed + (places - fixed + offset_by * (used - fixed)) % max(1, count - fixed)
        return jnp.zeros((count,), jnp.int32).at[order[jnp.where(places < fixed, places, moved)]].set(jnp.asarray(lengths, jnp.int32))

    lengths = jnp.where(number % 4 == 0, named(heavy_load, number // 4), named(ordinary, number - number // 4 - 1))
    mixed = jax.random.permutation(jax.random.fold_in(own, 3), count)
    donor, taker = mixed[0:count // 2 * 2:2], mixed[1:count // 2 * 2:2]
    room = jnp.minimum(lengths[donor] - 1, most - lengths[taker]) // 2
    room = jnp.where((donor == order[0]) | (taker == order[0]) | (lengths[taker] == 0), 0, jnp.maximum(room, 0))
    moved = jax.random.randint(jax.random.fold_in(own, 4), (count // 2,), 0, 1 << 20) % (room + 1)
    lengths = lengths.at[donor].add(-moved).at[taker].add(moved)
    items = jnp.searchsorted(jnp.cumsum(lengths), jnp.arange(rows * top), side="right").astype(jnp.int32)
    table = items.reshape(top, rows).T
    table = table[jax.random.permutation(jax.random.fold_in(own, 1), rows)]
    offset_by = jax.random.randint(jax.random.fold_in(own, 2), (rows, 1), 0, top)
    return jnp.take_along_axis(table, (jnp.arange(top)[None, :] + offset_by) % top, axis=1)


def portions_of(amount, total, bound, skew, full):
    portions = [(1 << 20) // math.isqrt(standing ** skew) + 1 for standing in range(1, amount + 1)]
    largest = bound if full else min(bound, max(-(-total // amount), total * portions[0] // sum(portions)))
    least = 1 if total - largest >= amount - 1 else 0
    holding, spare = [largest] + [least] * (amount - 1), total - largest - least * (amount - 1)
    while spare > 0:
        candidates = [i for i in range(1, amount) if holding[i] < largest] or [i for i in range(1, amount) if holding[i] < bound]
        whole, left = sum([portions[i] for i in candidates]), spare
        for i in candidates:
            addition = min(bound - holding[i], max(1, left * portions[i] // whole), spare)
            holding[i] = holding[i] + addition
            spare = spare - addition
    return np.array(holding)


def normal_values(key, shape, spread, limit, pieces=(), kind=jnp.bfloat16):
    drawn = spread * jax.random.normal(key, shape, jnp.float32)
    if pieces:
        drawn = drawn * shard_levels(key, shape, pieces, -0.22, 0.18)
    return jnp.clip(drawn, -limit, limit).astype(kind)


def setup_inputs(seed: int = 0, part: int = 0) -> dict:
    key_list = jax.random.split(jax.random.key(seed), 8)
    part_keys = jax.random.split(jax.random.fold_in(key_list[7], part), 8)
    tokens = normal_values(part_keys[0], (TOKENS, D), 1.0, 6.0, ((0, 64),))
    norm_gain = jnp.clip(1.0 + 0.18 * jax.random.normal(key_list[1], (D,), jnp.float32), 0.1, 1.9)
    w_gate = normal_values(key_list[2], (EXPERTS, D, FF), (D // 6) ** -0.5, 0.3125, ((0, 64), (2, 4)))
    w_up = normal_values(key_list[3], (EXPERTS, D, FF), (D // 6) ** -0.5, 0.3125, ((0, 64), (2, 4)))
    w_down = normal_values(key_list[4], (EXPERTS, FF, D), (FF * 4) ** -0.5, 0.09375, ((0, 64), (1, 4)))
    expert_ids_keys = jax.random.split(jax.random.fold_in(part_keys[5], 1), TOKENS // TOK_DEV)
    expert_ids_turns = jax.random.permutation(jax.random.fold_in(part_keys[5], 3), TOKENS // TOK_DEV)
    expert_ids = jax.vmap(lambda own, number: deal_out(jax.random.fold_in(part_keys[5], 2), own, number, TOK_DEV, EXPERTS, TOP_K, CAP, 1))(expert_ids_keys, expert_ids_turns).reshape((TOKENS, TOP_K))
    gate_weights = jnp.clip(0.1 + 0.9 * jax.random.uniform(part_keys[6], (TOKENS, TOP_K), jnp.float32) ** shard_levels(part_keys[6], (TOKENS, TOP_K), ((0, 64),), -0.2, 0.2), 0.1, 1.0)
    return {"tokens": tokens, "norm_gain": norm_gain, "w_gate": w_gate, "w_up": w_up, "w_down": w_down, "expert_ids": expert_ids, "gate_weights": gate_weights}


epsilon = 1e-06
clamp_limit = 7.0
swish_alpha = 1.702

def rms_norm(tokens, norm_gain):
    widened = tokens.astype(jnp.float32)
    scaled = widened * lax.rsqrt(lax.optimization_barrier(jnp.mean(widened * widened, axis=-1, keepdims=True)) + epsilon)
    return (scaled * norm_gain).astype(jnp.bfloat16)

def reference(tokens, norm_gain, w_gate, w_up, w_down, expert_ids, gate_weights):
    normed = rms_norm(tokens, norm_gain)
    src_ids = expert_ids.reshape(N_EP, TOK_DEV * TOP_K).astype(jnp.int32)
    onehot = (src_ids[:, :, None] == jnp.arange(EXPERTS, dtype=jnp.int32)[None, None, :]).astype(jnp.int32)
    before = jnp.cumsum(onehot, axis=1) - onehot
    slot_index = lax.optimization_barrier(jnp.sum(before * onehot, axis=2)).astype(jnp.int32)
    source = jnp.arange(N_EP, dtype=jnp.int32)[:, None]
    row_index = (src_ids * (N_EP * CAP) + source * CAP + slot_index).astype(jnp.int32)
    owner_tok = (source * TOK_DEV + jnp.arange(TOK_DEV * TOP_K, dtype=jnp.int32)[None, :] // TOP_K).astype(jnp.int32)
    slot_table = jnp.full((EXPERTS * N_EP * CAP,), TOKENS, jnp.int32)
    slot_table = slot_table.at[row_index.reshape(-1)].set(owner_tok.reshape(-1)).reshape(EXPERTS, N_EP * CAP)
    padded = jnp.concatenate([normed, jnp.zeros((1, D), jnp.bfloat16)], axis=0)

    def expert_fn(packed):
        slot_rows, gate_mat, up_mat, down_mat = packed
        expert_rows = padded[slot_rows]
        gate_pre = jnp.dot(expert_rows, gate_mat, preferred_element_type=jnp.float32)
        up_pre = jnp.dot(expert_rows, up_mat, preferred_element_type=jnp.float32)
        gated = jnp.minimum(gate_pre, clamp_limit)
        linear = jnp.clip(up_pre, -clamp_limit, clamp_limit)
        activated = (gated * jax.nn.sigmoid(swish_alpha * gated) * (linear + 1.0)).astype(jnp.bfloat16)
        act_blocks = activated.reshape(-1, N_TP, FF // N_TP).astype(jnp.float32)
        down_blocks = down_mat.reshape(N_TP, FF // N_TP, D).astype(jnp.float32)
        partial_value = jnp.einsum('rtf,tfd->rtd', act_blocks, down_blocks).astype(jnp.bfloat16)
        partial_value = lax.optimization_barrier(partial_value)
        return lax.optimization_barrier(jnp.sum(partial_value.astype(jnp.float32), axis=1)).astype(jnp.bfloat16)
    expert_out = lax.map(expert_fn, (slot_table, w_gate, w_up, w_down))
    picked = expert_out.reshape(EXPERTS * N_EP * CAP, D)[row_index.reshape(-1)]
    picked = picked.reshape(TOKENS, TOP_K, D).astype(jnp.float32)
    return lax.optimization_barrier(jnp.sum(picked * gate_weights[:, :, None], axis=1)).astype(jnp.bfloat16)
```

```python
import functools

import jax
import jax.numpy as jnp
from jax import lax
from jax.experimental import pallas as pl
from jax.experimental.pallas import tpu as pltpu
from jax.sharding import PartitionSpec as P

MESH = pl.DeviceIdType.MESH
BF16 = jnp.bfloat16
F32 = jnp.float32

epsilon = 1e-06
clamp_limit = 7.0
swish_alpha = 1.702

CORES = 2
PARTS = 3


def kernel(
    cfg,
    tok_ref,
    gain_ref,
    meta_ref,
    wg_hbm,
    wu_hbm,
    wd_hbm,
    out_ref,
    ag,
    agm,
    rs,
    rsend,
    grow,
    stg,
    part,
    relay,
    direct,
    pair,
    pair_in,
    y_own,
    y_out,
    y_sib,
    cbuf,
    back,
    wg,
    wu,
    wd,
    w_sem,
    ag_send,
    ag_recv,
    rs_send,
    rs_recv,
    sel_send,
    sel_recv,
    xg_send,
    xg_recv,
    xr_send,
    xr_recv,
    y_send,
    y_recv,
):
    nz, nx, cap, rows, cols, pad = cfg
    half = nz // 2
    sub = rows // PARTS
    ep = lax.axis_index("ep")
    x = lax.axis_index("tp")
    z, c = ep // CORES, ep % CORES
    f = 1 - 2 * c

    def wrap(v, n):
        return lax.rem(v + 2 * n, n)

    z_to = (
        {"ep": wrap(z + 1, nz) * CORES + c},
        {"ep": wrap(z - 1, nz) * CORES + c},
    )
    sib = {"ep": z * CORES + 1 - c}
    x_up, x_dn = {"tp": wrap(x + 1, nx)}, {"tp": wrap(x - 1, nx)}
    x_f, x_b = wrap(x + f, nx), wrap(x - f, nx)
    x_far = wrap(x + 2, nx)

    def reach(d):
        return half - jnp.where(c == d, 0, 1)

    def hops(d, j):
        if j == PARTS:
            return reach(d)
        return reach(d) - (sub * j) // (CORES * cap)

    def remote(src, dst, ssem, rsem, dev):
        return pltpu.make_async_remote_copy(
            src_ref=src, dst_ref=dst, send_sem=ssem, recv_sem=rsem,
            device_id=dev, device_id_type=MESH,
        )

    def ag_copy(d, h, j):
        ssem = ag_send.at[d, lax.rem(h, 2), j]
        if j == PARTS:
            return remote(agm.at[d, h], agm.at[d, h + 1], ssem, ag_recv.at[d, h + 1, j], z_to[d])
        win = pl.ds(j * sub, sub)
        return remote(
            ag.at[d, h, win], ag.at[d, h + 1, win], ssem, ag_recv.at[d, h + 1, j], z_to[d]
        )

    def rs_copy(d, h, j):
        win = pl.ds(j * sub, sub)
        par = lax.rem(h, 2)
        return remote(
            rsend.at[d, par, win], rs.at[d, h - 1, win],
            rs_send.at[d, par, j], rs_recv.at[d, h - 1, j], z_to[1 - d],
        )

    def sel_copy(h):
        return remote(
            stg.at[h], grow.at[x, h, pl.ds(2 * cap, 2 * cap)], sel_send.at[h], sel_recv.at[h], sib
        )

    def xg_copy(h, way):
        if way == 0:
            return remote(grow.at[x, h], grow.at[x, h], xg_send.at[h, 0], xg_recv.at[h, 0], x_up)
        if way == 1:
            return remote(grow.at[x, h], grow.at[x, h], xg_send.at[h, 1], xg_recv.at[h, 1], x_dn)
        return remote(
            grow.at[x_b, h], grow.at[x_b, h], xg_send.at[h, 2], xg_recv.at[h, 2], {"tp": x_f}
        )

    def xr_copy(h, way):
        if way == 0:
            return remote(
                part.at[h, x_far], relay.at[h], xr_send.at[h, 0], xr_recv.at[h, 0], {"tp": x_f}
            )
        if way == 1:
            return remote(
                part.at[h, x_b], direct.at[h], xr_send.at[h, 1], xr_recv.at[h, 1], {"tp": x_b}
            )
        return remote(
            pair.at[h], pair_in.at[h], xr_send.at[h, 2], xr_recv.at[h, 2], {"tp": x_f}
        )

    def y_copy(h):
        return remote(y_out.at[h], y_sib.at[h], y_send.at[h], y_recv.at[h], sib)

    weights = [
        pltpu.make_async_copy(src.at[0], dst, w_sem.at[k])
        for k, (src, dst) in enumerate(((wg_hbm, wg), (wu_hbm, wu), (wd_hbm, wd)))
    ]
    for copy in weights:
        copy.start()

    for d in range(2):
        for j in range(PARTS + 1):
            low = half - 1 - (0 if j == PARTS else (sub * j) // (CORES * cap))
            for h in range(max(low, 0), half + 1):
                if j < PARTS:
                    @pl.when(h >= hops(d, j))
                    def _():
                        rs[d, h, pl.ds(j * sub, sub)] = jnp.zeros((sub, cols), BF16)
                if h >= 1:
                    @pl.when(h > hops(d, j))
                    def _():
                        if j < PARTS:
                            ag[d, h, pl.ds(j * sub, sub)] = jnp.zeros((sub, cols), BF16)
                        else:
                            agm[d, h] = jnp.full((8, pad), -1.0, F32)

    barrier = pltpu.get_barrier_semaphore()
    for dev in (*z_to, sib, x_up, x_dn):
        pl.semaphore_signal(barrier, inc=1, device_id=dev, device_id_type=MESH)

    widened = tok_ref[...].astype(F32)
    scale = lax.rsqrt(jnp.mean(widened * widened, axis=-1, keepdims=True) + epsilon)
    mine = pl.ds(pl.multiple_of(x * cols, cols), cols)
    own_cols = tok_ref[:, mine].astype(F32) * scale
    own_cols = (own_cols * gain_ref[:, mine]).astype(BF16)

    meta = meta_ref[...]
    ids = meta[0:4].astype(jnp.int32)
    ahead = lax.shift_right_arithmetic(ids, 1) - z
    ahead = jnp.where(ahead < 0, ahead + nz, ahead)
    behind = jnp.where(ahead == 0, 0, nz - ahead)
    lane = lax.broadcasted_iota(jnp.int32, (pad, pad), 1)
    line = lax.broadcasted_iota(jnp.int32, (pad, pad), 0)
    for d, dist in enumerate((ahead, behind)):
        far = jnp.max(jnp.where(dist <= reach(d), dist, 0), axis=0, keepdims=True)
        far = jnp.where(lane[0:1] < rows, far, -1).astype(F32)
        by_lane = jnp.broadcast_to(far, (pad, pad))
        by_line = by_lane.T
        first = (by_line > by_lane) | ((by_line == by_lane) & (line < lane))
        rank_lane = jnp.sum(jnp.where(first, 1.0, 0.0), axis=0, keepdims=True)
        later = (by_lane > by_line) | ((by_lane == by_line) & (lane < line))
        rank_line = jnp.sum(jnp.where(later, 1.0, 0.0), axis=1, keepdims=True)
        order = jnp.where(rank_lane == line.astype(F32), 1.0, 0.0).astype(BF16)
        back_to = jnp.where(rank_line == lane.astype(F32), 1.0, 0.0).astype(BF16)
        ag[d, 0] = jnp.dot(
            order[:rows, :rows], own_cols, preferred_element_type=F32
        ).astype(BF16)
        agm[d, 0] = jnp.dot(meta.astype(BF16), back_to, preferred_element_type=F32)
        back[d] = back_to

    pl.semaphore_wait(barrier, 5)

    sub_line = lax.broadcasted_iota(jnp.int32, (2 * cap, pad), 0)
    own_slot = jnp.where(sub_line < cap, sub_line, sub_line - cap).astype(F32)

    def select(d, h):
        valid = h <= reach(d)
        if d == 1:
            valid = valid & (h >= 1)
        expert = jnp.where(sub_line < cap, ep, z * CORES + 1 - c)
        expert = jnp.where(valid, expert, -7).astype(F32)
        meta = agm[d, h]
        named = jnp.zeros((2 * cap, pad), F32)
        weight = jnp.zeros((2 * cap, pad), F32)
        for k in range(4):
            same = jnp.where(meta[k : k + 1] == expert, 1.0, 0.0)
            named = named + same
            weight = weight + same * meta[k + 4 : k + 5]
        before = jnp.where(
            lax.broadcasted_iota(jnp.int32, (pad, pad), 0)
            < lax.broadcasted_iota(jnp.int32, (pad, pad), 1),
            1.0, 0.0,
        ).astype(BF16)
        slot = jnp.dot(named.astype(BF16), before, preferred_element_type=F32)
        pick = jnp.where(slot == own_slot, named, 0.0)
        spread = (pick * weight).astype(BF16)
        eye = jnp.where(
            lax.broadcasted_iota(jnp.int32, (rows, pad), 0)
            == lax.broadcasted_iota(jnp.int32, (rows, pad), 1),
            1.0, 0.0,
        ).astype(BF16)
        cbuf[d, h] = lax.dot_general(
            eye, spread, (((1,), (1,)), ((), ())), preferred_element_type=F32
        ).astype(BF16)
        got = jnp.dot(
            pick.astype(BF16)[:, :rows], ag[d, h], preferred_element_type=F32
        ).astype(BF16)
        grow[x, h, pl.ds(d * cap, cap)] = got[:cap]
        stg[h, pl.ds(d * cap, cap)] = got[cap:]

    def dispatch(i, _):
        @pl.when(i <= half)
        def _():
            for j in (PARTS, *range(PARTS)):
                for d in range(2):
                    @pl.when((i >= 1) & (i <= hops(d, j)))
                    def _():
                        ag_copy(d, i - 1, j).wait_recv()

                    @pl.when(i < hops(d, j))
                    def _():
                        @pl.when(i >= 2)
                        def _():
                            ag_copy(d, i - 2, j).wait_send()

                        ag_copy(d, i, j).start()

        @pl.when(i >= 2)
        def _():
            h = i - 2
            remote(
                grow.at[x_b, h], grow.at[x_b, h], xg_send.at[h, 2], xg_recv.at[h, c], x_up
            ).wait_recv()
            xg_copy(h, 2).start()

        @pl.when((i >= 1) & (i <= half + 1))
        def _():
            h = i - 1
            sel_copy(h).wait_recv()
            xg_copy(h, 0).start()
            xg_copy(h, 1).start()

        @pl.when(i <= half)
        def _():
            select(0, i)
            select(1, i)
            sel_copy(i).start()

        return 0

    lax.fori_loop(0, half + 3, dispatch, 0)

    for copy in weights:
        copy.wait()

    def blend(d, h, j):
        win = pl.ds(j * sub, sub)
        mid = pl.ds(d * cap, cap)
        both = jnp.concatenate([y_own[h, mid], y_sib[h, mid]], axis=0)
        gain = jnp.dot(cbuf[d, h, win], both, preferred_element_type=F32)
        return rs[d, h, win].astype(F32) + gain

    def gather_back(i, _):
        @pl.when(i >= 3)
        def _():
            h = half - i + 3
            y_copy(h).wait_recv()
            for j in range(PARTS):
                for d in range(2):
                    @pl.when(h + 1 <= hops(d, j))
                    def _():
                        rs_copy(d, h + 1, j).wait_recv()

                    @pl.when(h + 2 <= hops(d, j))
                    def _():
                        rs_copy(d, h + 2, j).wait_send()

                    @pl.when(h <= hops(d, j))
                    def _():
                        rsend[d, lax.rem(h, 2), pl.ds(j * sub, sub)] = blend(d, h, j).astype(BF16)
                        rs_copy(d, h, j).start()

        @pl.when((i >= 2) & (i <= half + 2))
        def _():
            h = half - i + 2
            xr_copy(h, 1).wait_recv()
            xr_copy(h, 2).wait_recv()
            total = (
                part[h, x].astype(F32) + direct[h].astype(F32) + pair_in[h].astype(F32)
            ).astype(BF16)
            y_own[h] = total[: 2 * cap]
            y_out[h] = total[2 * cap :]
            y_copy(h).start()

        @pl.when((i >= 1) & (i <= half + 1))
        def _():
            h = half - i + 1
            xr_copy(h, 0).wait_recv()
            pair[h] = (part[h, x_f].astype(F32) + relay[h].astype(F32)).astype(BF16)
            xr_copy(h, 2).start()

        @pl.when(i <= half)
        def _():
            h = half - i
            remote(
                grow.at[x_f, h], grow.at[x_f, h], xg_send.at[h, 2], xg_recv.at[h, 1 - c], x_up
            ).wait_recv()
            xg_copy(h, 2).wait_recv()
            gate = jnp.zeros((4 * cap, wg.shape[1]), F32)
            up = jnp.zeros((4 * cap, wg.shape[1]), F32)
            for k in range(nx):
                block = grow[k, h]
                gate = gate + jnp.dot(
                    block, wg[pl.ds(k * cols, cols)], preferred_element_type=F32
                )
                up = up + jnp.dot(block, wu[pl.ds(k * cols, cols)], preferred_element_type=F32)
            gated = jnp.minimum(gate, clamp_limit)
            linear = jnp.clip(up, -clamp_limit, clamp_limit)
            active = (gated * jax.nn.sigmoid(swish_alpha * gated) * (linear + 1.0)).astype(BF16)
            for k in range(nx):
                part[h, k] = jnp.dot(
                    active, wd[:, pl.ds(k * cols, cols)], preferred_element_type=F32
                ).astype(BF16)
            xr_copy(h, 0).start()
            xr_copy(h, 1).start()

        return 0

    lax.fori_loop(0, half + 3, gather_back, 0)

    y_copy(0).wait_recv()
    total = jnp.zeros((rows, cols), F32)
    for d in range(2):
        for j in range(PARTS):
            @pl.when(1 <= hops(d, j))
            def _():
                rs_copy(d, 1, j).wait_recv()
        held = jnp.concatenate(
            [blend(d, 0, j).astype(BF16) for j in range(PARTS)], axis=0
        )
        total = total + jnp.dot(back[d, :rows, :rows], held, preferred_element_type=F32)
    out_ref[...] = total.astype(BF16)

    for d in range(2):
        for j in range(PARTS + 1):
            for k in (1, 2):
                @pl.when(hops(d, j) >= k)
                def _():
                    ag_copy(d, hops(d, j) - k, j).wait_send()
                if j < PARTS:
                    @pl.when(hops(d, j) >= k)
                    def _():
                        rs_copy(d, k, j).wait_send()

    def drain(h, _):
        sel_copy(h).wait_send()
        y_copy(h).wait_send()
        for way in range(3):
            xg_copy(h, way).wait_send()
            xr_copy(h, way).wait_send()
        return 0

    lax.fori_loop(0, half + 1, drain, 0)


def body(ep_count, tp_count, tokens, norm_gain, w_gate, w_up, w_down, expert_ids, gate_weights):
    rows, width = tokens.shape
    top = expert_ids.shape[1]
    experts = w_gate.shape[0] * ep_count
    cap = min(rows, rows * top * 4 // (3 * experts))
    cols = width // tp_count
    hidden = w_gate.shape[2]
    pad = -(-rows // 128) * 128
    steps = ep_count // CORES // 2 + 1
    meta = jnp.concatenate([expert_ids.astype(F32).T, gate_weights.T], axis=0)
    meta = jnp.pad(meta, ((0, 0), (0, pad - rows)), constant_values=-1.0)
    vmem = pl.BlockSpec(memory_space=pltpu.VMEM)
    hbm = pl.BlockSpec(memory_space=pl.ANY)
    dma = pltpu.SemaphoreType.DMA
    block = (4 * cap, cols)
    return pl.pallas_call(
        functools.partial(kernel, (ep_count // CORES, tp_count, cap, rows, cols, pad)),
        out_shape=jax.ShapeDtypeStruct((rows, cols), BF16),
        in_specs=[vmem, vmem, vmem, hbm, hbm, hbm],
        out_specs=vmem,
        scratch_shapes=[
            pltpu.VMEM((2, steps, rows, cols), BF16),
            pltpu.VMEM((2, steps, 8, pad), F32),
            pltpu.VMEM((2, steps, rows, cols), BF16),
            pltpu.VMEM((2, 2, rows, cols), BF16),
            pltpu.VMEM((tp_count, steps, *block), BF16),
            pltpu.VMEM((steps, 2 * cap, cols), BF16),
            pltpu.VMEM((steps, tp_count, *block), BF16),
            pltpu.VMEM((steps, *block), BF16),
            pltpu.VMEM((steps, *block), BF16),
            pltpu.VMEM((steps, *block), BF16),
            pltpu.VMEM((steps, *block), BF16),
            pltpu.VMEM((steps, 2 * cap, cols), BF16),
            pltpu.VMEM((steps, 2 * cap, cols), BF16),
            pltpu.VMEM((steps, 2 * cap, cols), BF16),
            pltpu.VMEM((2, steps, rows, 2 * cap), BF16),
            pltpu.VMEM((2, pad, pad), BF16),
            pltpu.VMEM((width, hidden), BF16),
            pltpu.VMEM((width, hidden), BF16),
            pltpu.VMEM((hidden, width), BF16),
            dma((3,)),
            dma((2, 2, PARTS + 1)),
            dma((2, steps, PARTS + 1)),
            dma((2, 2, PARTS)),
            dma((2, steps, PARTS)),
            dma((steps,)),
            dma((steps,)),
            dma((steps, 3)),
            dma((steps, 3)),
            dma((steps, 3)),
            dma((steps, 3)),
            dma((steps,)),
            dma((steps,)),
        ],
        compiler_params=pltpu.CompilerParams(
            collective_id=0, has_side_effects=True, vmem_limit_bytes=60 * 1024 * 1024
        ),
    )(tokens, norm_gain.reshape(1, width), meta, w_gate, w_up, w_down)


def solution(mesh):
    return jax.shard_map(
        functools.partial(body, mesh.shape["ep"], mesh.shape["tp"]),
        mesh=mesh,
        in_specs=(
            P(("grp", "ep"), None),
            P(),
            P("ep", None, "tp"),
            P("ep", None, "tp"),
            P("ep", "tp", None),
            P(("grp", "ep"), None),
            P(("grp", "ep"), None),
        ),
        out_specs=P(("grp", "ep"), "tp"),
        check_vma=False,
    )
```

```python
import functools

import jax
import jax.numpy as jnp
from jax import lax
from jax.experimental import pallas as pl
from jax.experimental.pallas import tpu as pltpu
from jax.sharding import PartitionSpec as P

MESH = pl.DeviceIdType.MESH
BF16 = jnp.bfloat16
F32 = jnp.float32

epsilon = 1e-06
clamp_limit = 7.0
swish_alpha = 1.702

CORES = 2
PARTS = 6


def kernel(
    cfg,
    tok_hbm,
    gain_ref,
    meta_ref,
    wg_hbm,
    wu_hbm,
    wd_hbm,
    out_ref,
    ag,
    agm,
    rs,
    rsend,
    grow,
    stg,
    part,
    relay,
    direct,
    pair,
    pair_in,
    y_own,
    y_out,
    y_sib,
    cbuf,
    gains,
    back,
    tok,
    wg,
    wu,
    wd,
    w_sem,
    ag_send,
    ag_recv,
    rs_send,
    rs_recv,
    sel_send,
    sel_recv,
    xg_send,
    xg_recv,
    xr_send,
    xr_recv,
    y_send,
    y_recv,
):
    nz, nx, cap, rows, cols, pad = cfg
    half = nz // 2
    sub = rows // PARTS
    ep = lax.axis_index("ep")
    x = lax.axis_index("tp")
    z, c = ep // CORES, ep % CORES
    f = 1 - 2 * c

    def wrap(v, n):
        return lax.rem(v + 2 * n, n)

    z_to = (
        {"ep": wrap(z + 1, nz) * CORES + c},
        {"ep": wrap(z - 1, nz) * CORES + c},
    )
    sib = {"ep": z * CORES + 1 - c}
    x_up, x_dn = {"tp": wrap(x + 1, nx)}, {"tp": wrap(x - 1, nx)}
    x_f, x_b = wrap(x + f, nx), wrap(x - f, nx)
    x_far = wrap(x + 2, nx)

    def reach(d):
        return half - jnp.where(c == d, 0, 1)

    def hops(d, j):
        if j == PARTS:
            return reach(d)
        return reach(d) - (sub * j) // (CORES * cap)

    def remote(src, dst, ssem, rsem, dev):
        return pltpu.make_async_remote_copy(
            src_ref=src, dst_ref=dst, send_sem=ssem, recv_sem=rsem,
            device_id=dev, device_id_type=MESH,
        )

    def ag_copy(d, h, j):
        ssem = ag_send.at[d, lax.rem(h, 2), j]
        if j == PARTS:
            return remote(agm.at[d, h], agm.at[d, h + 1], ssem, ag_recv.at[d, h + 1, j], z_to[d])
        win = pl.ds(j * sub, sub)
        return remote(
            ag.at[d, h, win], ag.at[d, h + 1, win], ssem, ag_recv.at[d, h + 1, j], z_to[d]
        )

    def rs_copy(d, h, j):
        win = pl.ds(j * sub, sub)
        par = lax.rem(h, 2)
        return remote(
            rsend.at[d, par, win], rs.at[d, h - 1, win],
            rs_send.at[d, par, j], rs_recv.at[d, h - 1, j], z_to[1 - d],
        )

    def sel_copy(h):
        return remote(
            stg.at[h], grow.at[x, h, pl.ds(2 * cap, 2 * cap)], sel_send.at[h], sel_recv.at[h], sib
        )

    def xg_copy(h, way):
        if way == 0:
            return remote(grow.at[x, h], grow.at[x, h], xg_send.at[h, 0], xg_recv.at[h, 0], x_up)
        if way == 1:
            return remote(grow.at[x, h], grow.at[x, h], xg_send.at[h, 1], xg_recv.at[h, 1], x_dn)
        return remote(
            grow.at[x_b, h], grow.at[x_b, h], xg_send.at[h, 2], xg_recv.at[h, 2], {"tp": x_f}
        )

    def xr_copy(h, way):
        if way == 0:
            return remote(
                part.at[h, x_far], relay.at[h], xr_send.at[h, 0], xr_recv.at[h, 0], {"tp": x_f}
            )
        if way == 1:
            return remote(
                part.at[h, x_b], direct.at[h], xr_send.at[h, 1], xr_recv.at[h, 1], {"tp": x_b}
            )
        return remote(
            pair.at[h], pair_in.at[h], xr_send.at[h, 2], xr_recv.at[h, 2], {"tp": x_f}
        )

    def y_copy(h):
        return remote(y_out.at[h], y_sib.at[h], y_send.at[h], y_recv.at[h], sib)

    barrier = pltpu.get_barrier_semaphore()
    for dev in (*z_to, sib, x_up, x_dn):
        pl.semaphore_signal(barrier, inc=1, device_id=dev, device_id_type=MESH)

    load = pltpu.make_async_copy(tok_hbm, tok, w_sem.at[3])
    load.start()
    weights = [
        pltpu.make_async_copy(src.at[0], dst, w_sem.at[k])
        for k, (src, dst) in enumerate(((wg_hbm, wg), (wu_hbm, wu), (wd_hbm, wd)))
    ]
    for copy in weights:
        copy.start()

    for d in range(2):
        for j in range(PARTS + 1):
            low = half - 1 - (0 if j == PARTS else (sub * j) // (CORES * cap))
            for h in range(max(low, 0), half + 1):
                if j < PARTS:
                    @pl.when(h >= hops(d, j))
                    def _():
                        rs[d, h, pl.ds(j * sub, sub)] = jnp.zeros((sub, cols), BF16)
                if h >= 1:
                    @pl.when(h > hops(d, j))
                    def _():
                        if j < PARTS:
                            ag[d, h, pl.ds(j * sub, sub)] = jnp.zeros((sub, cols), BF16)
                        else:
                            agm[d, h] = jnp.full((8, pad), -1.0, F32)

    load.wait()
    widened = tok[...].astype(F32)
    scale = lax.rsqrt(jnp.mean(widened * widened, axis=-1, keepdims=True) + epsilon)
    mine = pl.ds(pl.multiple_of(x * cols, cols), cols)
    own_cols = tok[:, mine].astype(F32) * scale
    own_cols = (own_cols * gain_ref[:, mine]).astype(BF16)

    meta = meta_ref[...]
    ids = meta[0:4].astype(jnp.int32)
    ahead = lax.shift_right_arithmetic(ids, 1) - z
    ahead = jnp.where(ahead < 0, ahead + nz, ahead)
    behind = jnp.where(ahead == 0, 0, nz - ahead)
    lane = lax.broadcasted_iota(jnp.int32, (pad, pad), 1)
    line = lax.broadcasted_iota(jnp.int32, (pad, pad), 0)
    for d, dist in enumerate((ahead, behind)):
        far = jnp.max(jnp.where(dist <= reach(d), dist, 0), axis=0, keepdims=True)
        far = jnp.where(lane[0:1] < rows, far, -1).astype(F32)
        by_lane = jnp.broadcast_to(far, (pad, pad))
        by_line = by_lane.T
        first = (by_line > by_lane) | ((by_line == by_lane) & (line < lane))
        rank_lane = jnp.sum(jnp.where(first, 1.0, 0.0), axis=0, keepdims=True)
        later = (by_lane > by_line) | ((by_lane == by_line) & (lane < line))
        rank_line = jnp.sum(jnp.where(later, 1.0, 0.0), axis=1, keepdims=True)
        order = jnp.where(rank_lane == line.astype(F32), 1.0, 0.0).astype(BF16)
        back_to = jnp.where(rank_line == lane.astype(F32), 1.0, 0.0).astype(BF16)
        ag[d, 0] = jnp.dot(
            order[:rows, :rows], own_cols, preferred_element_type=F32
        ).astype(BF16)
        agm[d, 0] = jnp.dot(meta.astype(BF16), back_to, preferred_element_type=F32)
        back[d] = back_to

    pl.semaphore_wait(barrier, 5)

    sub_line = lax.broadcasted_iota(jnp.int32, (2 * cap, pad), 0)
    own_slot = jnp.where(sub_line < cap, sub_line, sub_line - cap).astype(F32)

    def select(d, h):
        valid = h <= reach(d)
        if d == 1:
            valid = valid & (h >= 1)
        expert = jnp.where(sub_line < cap, ep, z * CORES + 1 - c)
        expert = jnp.where(valid, expert, -7).astype(F32)
        meta = agm[d, h]
        named = jnp.zeros((2 * cap, pad), F32)
        weight = jnp.zeros((2 * cap, pad), F32)
        for k in range(4):
            same = jnp.where(meta[k : k + 1] == expert, 1.0, 0.0)
            named = named + same
            weight = weight + same * meta[k + 4 : k + 5]
        before = jnp.where(
            lax.broadcasted_iota(jnp.int32, (pad, pad), 0)
            < lax.broadcasted_iota(jnp.int32, (pad, pad), 1),
            1.0, 0.0,
        ).astype(BF16)
        slot = jnp.dot(named.astype(BF16), before, preferred_element_type=F32)
        pick = jnp.where(slot == own_slot, named, 0.0)
        spread = (pick * weight).astype(BF16)
        eye = jnp.where(
            lax.broadcasted_iota(jnp.int32, (rows, pad), 0)
            == lax.broadcasted_iota(jnp.int32, (rows, pad), 1),
            1.0, 0.0,
        ).astype(BF16)
        cbuf[d, h] = lax.dot_general(
            eye, spread, (((1,), (1,)), ((), ())), preferred_element_type=F32
        ).astype(BF16)
        got = jnp.dot(
            pick.astype(BF16)[:, :rows], ag[d, h], preferred_element_type=F32
        ).astype(BF16)
        grow[x, h, pl.ds(d * cap, cap)] = got[:cap]
        stg[h, pl.ds(d * cap, cap)] = got[cap:]

    def dispatch(i, _):
        @pl.when(i <= half)
        def _():
            for j in (PARTS, *range(PARTS)):
                for d in range(2):
                    @pl.when((i >= 1) & (i <= hops(d, j)))
                    def _():
                        ag_copy(d, i - 1, j).wait_recv()

                    @pl.when(i < hops(d, j))
                    def _():
                        @pl.when(i >= 2)
                        def _():
                            ag_copy(d, i - 2, j).wait_send()

                        ag_copy(d, i, j).start()

        @pl.when((i >= 1) & (i <= half + 1))
        def _():
            h = i - 1
            sel_copy(h).wait_recv()
            xg_copy(h, 0).start()
            xg_copy(h, 1).start()

        @pl.when(i <= half)
        def _():
            select(0, i)
            select(1, i)
            sel_copy(i).start()

        @pl.when(i >= 2)
        def _():
            h = i - 2
            remote(
                grow.at[x_b, h], grow.at[x_b, h], xg_send.at[h, 2], xg_recv.at[h, c], x_up
            ).wait_recv()
            xg_copy(h, 2).start()

        return 0

    lax.fori_loop(0, half + 3, dispatch, 0)

    for copy in weights:
        copy.wait()

    def spread_out(h):
        for d in range(2):
            mid = pl.ds(d * cap, cap)
            both = jnp.concatenate([y_own[h, mid], y_sib[h, mid]], axis=0)
            gains[d] = jnp.dot(cbuf[d, h], both, preferred_element_type=F32)

    def blend(d, h, j):
        win = pl.ds(j * sub, sub)
        return rs[d, h, win].astype(F32) + gains[d, win]

    def gather_back(i, _):
        @pl.when(i >= 3)
        def _():
            h = half - i + 3
            y_copy(h).wait_recv()
            spread_out(h)
            for j in range(PARTS):
                for d in range(2):
                    @pl.when(h + 1 <= hops(d, j))
                    def _():
                        rs_copy(d, h + 1, j).wait_recv()

                    @pl.when(h + 2 <= hops(d, j))
                    def _():
                        rs_copy(d, h + 2, j).wait_send()

                    @pl.when(h <= hops(d, j))
                    def _():
                        rsend[d, lax.rem(h, 2), pl.ds(j * sub, sub)] = blend(d, h, j).astype(BF16)
                        rs_copy(d, h, j).start()

        @pl.when(i <= half)
        def _():
            h = half - i
            remote(
                grow.at[x_f, h], grow.at[x_f, h], xg_send.at[h, 2], xg_recv.at[h, 1 - c], x_up
            ).wait_recv()
            xg_copy(h, 2).wait_recv()
            gate = jnp.zeros((4 * cap, wg.shape[1]), F32)
            up = jnp.zeros((4 * cap, wg.shape[1]), F32)
            for k in range(nx):
                block = grow[k, h]
                gate = gate + jnp.dot(
                    block, wg[pl.ds(k * cols, cols)], preferred_element_type=F32
                )
                up = up + jnp.dot(block, wu[pl.ds(k * cols, cols)], preferred_element_type=F32)
            gated = jnp.minimum(gate, clamp_limit)
            linear = jnp.clip(up, -clamp_limit, clamp_limit)
            active = (gated * jax.nn.sigmoid(swish_alpha * gated) * (linear + 1.0)).astype(BF16)
            for k in range(nx):
                part[h, k] = jnp.dot(
                    active, wd[:, pl.ds(k * cols, cols)], preferred_element_type=F32
                ).astype(BF16)
            xr_copy(h, 0).start()
            xr_copy(h, 1).start()

        @pl.when((i >= 1) & (i <= half + 1))
        def _():
            h = half - i + 1
            xr_copy(h, 0).wait_recv()
            pair[h] = (part[h, x_f].astype(F32) + relay[h].astype(F32)).astype(BF16)
            xr_copy(h, 2).start()

        @pl.when((i >= 2) & (i <= half + 2))
        def _():
            h = half - i + 2
            xr_copy(h, 1).wait_recv()
            xr_copy(h, 2).wait_recv()
            total = (
                part[h, x].astype(F32) + direct[h].astype(F32) + pair_in[h].astype(F32)
            ).astype(BF16)
            y_own[h] = total[: 2 * cap]
            y_out[h] = total[2 * cap :]
            y_copy(h).start()

        return 0

    lax.fori_loop(0, half + 3, gather_back, 0)

    y_copy(0).wait_recv()
    spread_out(0)
    total = jnp.zeros((rows, cols), F32)
    for d in range(2):
        for j in range(PARTS):
            @pl.when(1 <= hops(d, j))
            def _():
                rs_copy(d, 1, j).wait_recv()
        held = jnp.concatenate(
            [blend(d, 0, j).astype(BF16) for j in range(PARTS)], axis=0
        )
        total = total + jnp.dot(back[d, :rows, :rows], held, preferred_element_type=F32)
    out_ref[...] = total.astype(BF16)

    for d in range(2):
        for j in range(PARTS + 1):
            for k in (1, 2):
                @pl.when(hops(d, j) >= k)
                def _():
                    ag_copy(d, hops(d, j) - k, j).wait_send()
                if j < PARTS:
                    @pl.when(hops(d, j) >= k)
                    def _():
                        rs_copy(d, k, j).wait_send()

    def drain(h, _):
        sel_copy(h).wait_send()
        y_copy(h).wait_send()
        for way in range(3):
            xg_copy(h, way).wait_send()
            xr_copy(h, way).wait_send()
        return 0

    lax.fori_loop(0, half + 1, drain, 0)


def body(ep_count, tp_count, tokens, norm_gain, w_gate, w_up, w_down, expert_ids, gate_weights):
    rows, width = tokens.shape
    top = expert_ids.shape[1]
    experts = w_gate.shape[0] * ep_count
    cap = min(rows, rows * top * 4 // (3 * experts))
    cols = width // tp_count
    hidden = w_gate.shape[2]
    pad = -(-rows // 128) * 128
    steps = ep_count // CORES // 2 + 1
    meta = jnp.concatenate([expert_ids.astype(F32).T, gate_weights.T], axis=0)
    meta = jnp.pad(meta, ((0, 0), (0, pad - rows)), constant_values=-1.0)
    vmem = pl.BlockSpec(memory_space=pltpu.VMEM)
    hbm = pl.BlockSpec(memory_space=pl.ANY)
    dma = pltpu.SemaphoreType.DMA
    block = (4 * cap, cols)
    return pl.pallas_call(
        functools.partial(kernel, (ep_count // CORES, tp_count, cap, rows, cols, pad)),
        out_shape=jax.ShapeDtypeStruct((rows, cols), BF16),
        in_specs=[hbm, vmem, vmem, hbm, hbm, hbm],
        out_specs=vmem,
        scratch_shapes=[
            pltpu.VMEM((2, steps, rows, cols), BF16),
            pltpu.VMEM((2, steps, 8, pad), F32),
            pltpu.VMEM((2, steps, rows, cols), BF16),
            pltpu.VMEM((2, 2, rows, cols), BF16),
            pltpu.VMEM((tp_count, steps, *block), BF16),
            pltpu.VMEM((steps, 2 * cap, cols), BF16),
            pltpu.VMEM((steps, tp_count, *block), BF16),
            pltpu.VMEM((steps, *block), BF16),
            pltpu.VMEM((steps, *block), BF16),
            pltpu.VMEM((steps, *block), BF16),
            pltpu.VMEM((steps, *block), BF16),
            pltpu.VMEM((steps, 2 * cap, cols), BF16),
            pltpu.VMEM((steps, 2 * cap, cols), BF16),
            pltpu.VMEM((steps, 2 * cap, cols), BF16),
            pltpu.VMEM((2, steps, rows, 2 * cap), BF16),
            pltpu.VMEM((2, rows, cols), F32),
            pltpu.VMEM((2, pad, pad), BF16),
            pltpu.VMEM((rows, width), BF16),
            pltpu.VMEM((width, hidden), BF16),
            pltpu.VMEM((width, hidden), BF16),
            pltpu.VMEM((hidden, width), BF16),
            dma((4,)),
            dma((2, 2, PARTS + 1)),
            dma((2, steps, PARTS + 1)),
            dma((2, 2, PARTS)),
            dma((2, steps, PARTS)),
            dma((steps,)),
            dma((steps,)),
            dma((steps, 3)),
            dma((steps, 3)),
            dma((steps, 3)),
            dma((steps, 3)),
            dma((steps,)),
            dma((steps,)),
        ],
        compiler_params=pltpu.CompilerParams(
            collective_id=0, has_side_effects=True, vmem_limit_bytes=60 * 1024 * 1024
        ),
    )(tokens, norm_gain.reshape(1, width), meta, w_gate, w_up, w_down)


def solution(mesh):
    return jax.shard_map(
        functools.partial(body, mesh.shape["ep"], mesh.shape["tp"]),
        mesh=mesh,
        in_specs=(
            P(("grp", "ep"), None),
            P(),
            P("ep", None, "tp"),
            P("ep", None, "tp"),
            P("ep", "tp", None),
            P(("grp", "ep"), None),
            P(("grp", "ep"), None),
        ),
        out_specs=P(("grp", "ep"), "tp"),
        check_vma=False,
    )
```

```python
import functools

import jax
import jax.numpy as jnp
from jax import lax
from jax.experimental import pallas as pl
from jax.experimental.pallas import tpu as pltpu
from jax.sharding import PartitionSpec as P

MESH = pl.DeviceIdType.MESH
BF16 = jnp.bfloat16
F32 = jnp.float32

epsilon = 1e-06
clamp_limit = 7.0
swish_alpha = 1.702

CORES = 2
PARTS = 6


def kernel(
    cfg,
    tok_hbm,
    gain_ref,
    meta_ref,
    wg_hbm,
    wu_hbm,
    wd_hbm,
    out_ref,
    ag,
    agm,
    rs,
    rsend,
    grow,
    stg,
    part,
    in_own,
    in_sib,
    cbuf,
    gains,
    back,
    tok,
    wg,
    wu,
    wd,
    w_sem,
    ag_send,
    ag_recv,
    rs_send,
    rs_recv,
    xg_send,
    xg_recv,
    xr_send,
    xr_recv,
):
    nz, nx, cap, rows, cols, pad = cfg
    half = nz // 2
    sub = rows // PARTS
    ep = lax.axis_index("ep")
    x = lax.axis_index("tp")
    z, c = ep // CORES, ep % CORES

    def wrap(v, n):
        return lax.rem(v + 2 * n, n)

    z_to = (
        {"ep": wrap(z + 1, nz) * CORES + c},
        {"ep": wrap(z - 1, nz) * CORES + c},
    )
    sib = z * CORES + 1 - c
    near, far_side = pl.ds(0, 2 * cap), pl.ds(2 * cap, 2 * cap)

    peers = [{"tp": wrap(x + r, nx)} for r in range(1, nx)]
    peers += [{"tp": wrap(x + r, nx), "ep": sib} for r in range(nx)]

    def reach(d):
        return half - jnp.where(c == d, 0, 1)

    def hops(d, j):
        if j == PARTS:
            return reach(d)
        return reach(d) - (sub * j) // (CORES * cap)

    def remote(src, dst, ssem, rsem, dev):
        return pltpu.make_async_remote_copy(
            src_ref=src, dst_ref=dst, send_sem=ssem, recv_sem=rsem,
            device_id=dev, device_id_type=MESH,
        )

    def ag_copy(d, h, j):
        ssem = ag_send.at[d, lax.rem(h, 2), j]
        if j == PARTS:
            return remote(agm.at[d, h], agm.at[d, h + 1], ssem, ag_recv.at[d, h + 1, j], z_to[d])
        win = pl.ds(j * sub, sub)
        return remote(
            ag.at[d, h, win], ag.at[d, h + 1, win], ssem, ag_recv.at[d, h + 1, j], z_to[d]
        )

    def rs_copy(d, h, j):
        win = pl.ds(j * sub, sub)
        par = lax.rem(h, 2)
        return remote(
            rsend.at[d, par, win], rs.at[d, h - 1, win],
            rs_send.at[d, par, j], rs_recv.at[d, h - 1, j], z_to[1 - d],
        )

    def live(base, core, last):
        if last:
            return pl.ds(pl.multiple_of(base + core * cap, cap), cap)
        return pl.ds(base, 2 * cap)

    def xg_copy(h, n, last):
        own = n < nx - 1
        src = grow.at[x, h, live(0, c, last)] if own else stg.at[h, live(0, c, last)]
        dst = grow.at[x, h, live(0 if own else 2 * cap, c, last)]
        return remote(src, dst, xg_send.at[h, n], xg_recv.at[h, n], peers[n])

    def xr_copy(h, n, last):
        own = n < nx - 1
        to = wrap(x + n + 1, nx) if own else wrap(x + n + 1 - nx, nx)
        core = c if own else 1 - c
        src = part.at[h, to, live(0 if own else 2 * cap, core, last)]
        dst = in_own.at[h, n] if own else in_sib.at[h, n + 1 - nx]
        return remote(
            src, dst.at[live(0, core, last)], xr_send.at[h, n], xr_recv.at[h, n], peers[n]
        )

    def for_peers(copy, h, act):
        @pl.when(h == half)
        def _():
            for n in range(len(peers)):
                act(copy(h, n, True))

        @pl.when(h != half)
        def _():
            for n in range(len(peers)):
                act(copy(h, n, False))

    def start(copy):
        copy.start()

    def arrived(copy):
        copy.wait_recv()

    def left(copy):
        copy.wait_send()

    barrier = pltpu.get_barrier_semaphore()
    for dev in (*z_to, *peers):
        pl.semaphore_signal(barrier, inc=1, device_id=dev, device_id_type=MESH)

    load = pltpu.make_async_copy(tok_hbm, tok, w_sem.at[3])
    load.start()
    weights = [
        pltpu.make_async_copy(src.at[0], dst, w_sem.at[k])
        for k, (src, dst) in enumerate(((wg_hbm, wg), (wu_hbm, wu), (wd_hbm, wd)))
    ]
    for copy in weights:
        copy.start()

    idle = jnp.zeros((cap, cols), BF16)
    for r in range(nx):
        grow[r, half, live(0, 1 - c, True)] = idle
        grow[r, half, live(2 * cap, c, True)] = idle
        in_sib[half, r, live(0, 1 - c, True)] = idle
        if r < nx - 1:
            in_own[half, r, live(0, 1 - c, True)] = idle
    for d in range(2):
        for j in range(PARTS + 1):
            low = half - 1 - (0 if j == PARTS else (sub * j) // (CORES * cap))
            for h in range(max(low, 0), half + 1):
                if j < PARTS:
                    @pl.when(h >= hops(d, j))
                    def _():
                        rs[d, h, pl.ds(j * sub, sub)] = jnp.zeros((sub, cols), BF16)
                if h >= 1:
                    @pl.when(h > hops(d, j))
                    def _():
                        if j < PARTS:
                            ag[d, h, pl.ds(j * sub, sub)] = jnp.zeros((sub, cols), BF16)
                        else:
                            agm[d, h] = jnp.full((8, pad), -1.0, BF16)

    meta = meta_ref[...]
    ids = meta[0:4].astype(jnp.int32)
    ahead = lax.shift_right_arithmetic(ids, 1) - z
    ahead = jnp.where(ahead < 0, ahead + nz, ahead)
    behind = jnp.where(ahead == 0, 0, nz - ahead)
    lane = lax.broadcasted_iota(jnp.int32, (pad, pad), 1)
    line = lax.broadcasted_iota(jnp.int32, (pad, pad), 0)
    orders = []
    for d, dist in enumerate((ahead, behind)):
        far = jnp.max(jnp.where(dist <= reach(d), dist, 0), axis=0, keepdims=True)
        far = jnp.where(lane[0:1] < rows, far, -1).astype(F32)
        by_lane = jnp.broadcast_to(far, (pad, pad))
        by_line = by_lane.T
        first = (by_line > by_lane) | ((by_line == by_lane) & (line < lane))
        rank_lane = jnp.sum(jnp.where(first, 1.0, 0.0), axis=0, keepdims=True)
        later = (by_lane > by_line) | ((by_lane == by_line) & (lane < line))
        rank_line = jnp.sum(jnp.where(later, 1.0, 0.0), axis=1, keepdims=True)
        order = jnp.where(rank_lane == line.astype(F32), 1.0, 0.0).astype(BF16)
        back_to = jnp.where(rank_line == lane.astype(F32), 1.0, 0.0).astype(BF16)
        orders.append(order[:rows, :rows])
        agm[d, 0] = jnp.dot(
            meta.astype(BF16), back_to, preferred_element_type=F32
        ).astype(BF16)
        back[d] = back_to

    load.wait()
    widened = tok[...].astype(F32)
    scale = lax.rsqrt(jnp.mean(widened * widened, axis=-1, keepdims=True) + epsilon)
    mine = pl.ds(pl.multiple_of(x * cols, cols), cols)
    own_cols = tok[:, mine].astype(F32) * scale
    own_cols = (own_cols * gain_ref[:, mine]).astype(BF16)
    for d in range(2):
        ag[d, 0] = jnp.dot(orders[d], own_cols, preferred_element_type=F32).astype(BF16)

    pl.semaphore_wait(barrier, 2 + len(peers))

    sub_line = lax.broadcasted_iota(jnp.int32, (2 * cap, pad), 0)
    own_slot = jnp.where(sub_line < cap, sub_line, sub_line - cap).astype(F32)

    def select(d, h):
        valid = h <= reach(d)
        if d == 1:
            valid = valid & (h >= 1)
        expert = jnp.where(sub_line < cap, ep, sib)
        expert = jnp.where(valid, expert, -7).astype(F32)
        meta = agm[d, h].astype(F32)
        named = jnp.zeros((2 * cap, pad), F32)
        weight = jnp.zeros((2 * cap, pad), F32)
        for k in range(4):
            same = jnp.where(meta[k : k + 1] == expert, 1.0, 0.0)
            named = named + same
            weight = weight + same * meta[k + 4 : k + 5]
        before = jnp.where(
            lax.broadcasted_iota(jnp.int32, (pad, pad), 0)
            < lax.broadcasted_iota(jnp.int32, (pad, pad), 1),
            1.0, 0.0,
        ).astype(BF16)
        slot = jnp.dot(named.astype(BF16), before, preferred_element_type=F32)
        pick = jnp.where(slot == own_slot, named, 0.0)
        spread = (pick * weight).astype(BF16)
        eye = jnp.where(
            lax.broadcasted_iota(jnp.int32, (rows, pad), 0)
            == lax.broadcasted_iota(jnp.int32, (rows, pad), 1),
            1.0, 0.0,
        ).astype(BF16)
        cbuf[d, h] = lax.dot_general(
            eye, spread, (((1,), (1,)), ((), ())), preferred_element_type=F32
        ).astype(BF16)
        got = jnp.dot(
            pick.astype(BF16)[:, :rows], ag[d, h], preferred_element_type=F32
        ).astype(BF16)
        grow[x, h, pl.ds(d * cap, cap)] = got[:cap]
        stg[h, pl.ds(d * cap, cap)] = got[cap:]

    def dispatch(i, _):
        for j in (PARTS, *range(PARTS)):
            for d in range(2):
                @pl.when((i >= 1) & (i <= hops(d, j)))
                def _():
                    ag_copy(d, i - 1, j).wait_recv()

                @pl.when(i < hops(d, j))
                def _():
                    @pl.when(i >= 2)
                    def _():
                        ag_copy(d, i - 2, j).wait_send()

                    ag_copy(d, i, j).start()

        select(0, i)
        select(1, i)
        for_peers(xg_copy, i, start)
        return 0

    lax.fori_loop(0, half + 1, dispatch, 0)

    for copy in weights:
        copy.wait()

    def spread_out(h):
        for_peers(xr_copy, h, arrived)
        y_own = part[h, x, near].astype(F32)
        y_sib = jnp.zeros_like(y_own)
        for r in range(nx):
            if r < nx - 1:
                y_own = y_own + in_own[h, r].astype(F32)
            y_sib = y_sib + in_sib[h, r].astype(F32)
        y_own, y_sib = y_own.astype(BF16), y_sib.astype(BF16)
        for d in range(2):
            both = jnp.concatenate(
                [y_own[d * cap : (d + 1) * cap], y_sib[d * cap : (d + 1) * cap]], axis=0
            )
            gains[d] = jnp.dot(cbuf[d, h], both, preferred_element_type=F32)

    def blend(d, h, j):
        win = pl.ds(j * sub, sub)
        return rs[d, h, win].astype(F32) + gains[d, win]

    def gather_back(i, _):
        @pl.when(i >= 2)
        def _():
            h = half - i + 2
            spread_out(h)
            for j in range(PARTS):
                for d in range(2):
                    @pl.when(h + 1 <= hops(d, j))
                    def _():
                        rs_copy(d, h + 1, j).wait_recv()

                    @pl.when(h + 2 <= hops(d, j))
                    def _():
                        rs_copy(d, h + 2, j).wait_send()

                    @pl.when(h <= hops(d, j))
                    def _():
                        rsend[d, lax.rem(h, 2), pl.ds(j * sub, sub)] = blend(d, h, j).astype(BF16)
                        rs_copy(d, h, j).start()

        @pl.when(i <= half)
        def _():
            h = half - i
            for_peers(xg_copy, h, arrived)
            gate = jnp.zeros((4 * cap, wg.shape[1]), F32)
            up = jnp.zeros((4 * cap, wg.shape[1]), F32)
            for k in range(nx):
                block = grow[k, h]
                gate = gate + jnp.dot(
                    block, wg[pl.ds(k * cols, cols)], preferred_element_type=F32
                )
                up = up + jnp.dot(block, wu[pl.ds(k * cols, cols)], preferred_element_type=F32)
            gated = jnp.minimum(gate, clamp_limit)
            linear = jnp.clip(up, -clamp_limit, clamp_limit)
            active = (gated * jax.nn.sigmoid(swish_alpha * gated) * (linear + 1.0)).astype(BF16)
            for k in range(nx):
                part[h, k] = jnp.dot(
                    active, wd[:, pl.ds(k * cols, cols)], preferred_element_type=F32
                ).astype(BF16)
            for_peers(xr_copy, h, start)

        return 0

    lax.fori_loop(0, half + 2, gather_back, 0)

    spread_out(0)
    total = jnp.zeros((rows, cols), F32)
    for d in range(2):
        for j in range(PARTS):
            @pl.when(1 <= hops(d, j))
            def _():
                rs_copy(d, 1, j).wait_recv()
        held = jnp.concatenate(
            [blend(d, 0, j).astype(BF16) for j in range(PARTS)], axis=0
        )
        total = total + jnp.dot(back[d, :rows, :rows], held, preferred_element_type=F32)
    out_ref[...] = total.astype(BF16)

    for d in range(2):
        for j in range(PARTS + 1):
            for k in (1, 2):
                @pl.when(hops(d, j) >= k)
                def _():
                    ag_copy(d, hops(d, j) - k, j).wait_send()
                if j < PARTS:
                    @pl.when(hops(d, j) >= k)
                    def _():
                        rs_copy(d, k, j).wait_send()

    def drain(h, _):
        for_peers(xg_copy, h, left)
        for_peers(xr_copy, h, left)
        return 0

    lax.fori_loop(0, half + 1, drain, 0)


def body(ep_count, tp_count, tokens, norm_gain, w_gate, w_up, w_down, expert_ids, gate_weights):
    rows, width = tokens.shape
    top = expert_ids.shape[1]
    experts = w_gate.shape[0] * ep_count
    cap = min(rows, rows * top * 4 // (3 * experts))
    cols = width // tp_count
    hidden = w_gate.shape[2]
    pad = -(-rows // 128) * 128
    steps = ep_count // CORES // 2 + 1
    meta = jnp.concatenate([expert_ids.astype(F32).T, gate_weights.T], axis=0)
    meta = jnp.pad(meta, ((0, 0), (0, pad - rows)), constant_values=-1.0)
    vmem = pl.BlockSpec(memory_space=pltpu.VMEM)
    hbm = pl.BlockSpec(memory_space=pl.ANY)
    dma = pltpu.SemaphoreType.DMA
    block = (4 * cap, cols)
    return pl.pallas_call(
        functools.partial(kernel, (ep_count // CORES, tp_count, cap, rows, cols, pad)),
        out_shape=jax.ShapeDtypeStruct((rows, cols), BF16),
        in_specs=[hbm, vmem, vmem, hbm, hbm, hbm],
        out_specs=vmem,
        scratch_shapes=[
            pltpu.VMEM((2, steps, rows, cols), BF16),
            pltpu.VMEM((2, steps, 8, pad), BF16),
            pltpu.VMEM((2, steps, rows, cols), BF16),
            pltpu.VMEM((2, 2, rows, cols), BF16),
            pltpu.VMEM((tp_count, steps, *block), BF16),
            pltpu.VMEM((steps, 2 * cap, cols), BF16),
            pltpu.VMEM((steps, tp_count, *block), BF16),
            pltpu.VMEM((steps, tp_count - 1, 2 * cap, cols), BF16),
            pltpu.VMEM((steps, tp_count, 2 * cap, cols), BF16),
            pltpu.VMEM((2, steps, rows, 2 * cap), BF16),
            pltpu.VMEM((2, rows, cols), F32),
            pltpu.VMEM((2, pad, pad), BF16),
            pltpu.VMEM((rows, width), BF16),
            pltpu.VMEM((width, hidden), BF16),
            pltpu.VMEM((width, hidden), BF16),
            pltpu.VMEM((hidden, width), BF16),
            dma((4,)),
            dma((2, 2, PARTS + 1)),
            dma((2, steps, PARTS + 1)),
            dma((2, 2, PARTS)),
            dma((2, steps, PARTS)),
            dma((steps, 2 * tp_count - 1)),
            dma((steps, 2 * tp_count - 1)),
            dma((steps, 2 * tp_count - 1)),
            dma((steps, 2 * tp_count - 1)),
        ],
        compiler_params=pltpu.CompilerParams(
            collective_id=0, has_side_effects=True, vmem_limit_bytes=60 * 1024 * 1024
        ),
    )(tokens, norm_gain.reshape(1, width), meta, w_gate, w_up, w_down)


def solution(mesh):
    return jax.shard_map(
        functools.partial(body, mesh.shape["ep"], mesh.shape["tp"]),
        mesh=mesh,
        in_specs=(
            P(("grp", "ep"), None),
            P(),
            P("ep", None, "tp"),
            P("ep", None, "tp"),
            P("ep", "tp", None),
            P(("grp", "ep"), None),
            P(("grp", "ep"), None),
        ),
        out_specs=P(("grp", "ep"), "tp"),
        check_vma=False,
    )
```

```python
import functools

import jax
import jax.numpy as jnp
from jax import lax
from jax.experimental import pallas as pl
from jax.experimental.pallas import tpu as pltpu
from jax.sharding import PartitionSpec as P

MESH = pl.DeviceIdType.MESH
BF16 = jnp.bfloat16
F32 = jnp.float32

epsilon = 1e-06
clamp_limit = 7.0
swish_alpha = 1.702

CORES = 2
PARTS = 6


def kernel(
    cfg,
    tok_hbm,
    gain_hbm,
    ids_hbm,
    gate_hbm,
    wg_hbm,
    wu_hbm,
    wd_hbm,
    out_ref,
    ag,
    agm,
    rs,
    rsend,
    grow,
    stg,
    part,
    inbox,
    cbuf,
    gains,
    back,
    tok,
    gain,
    ids_in,
    gate_in,
    meta_in,
    wg,
    wu,
    wd,
    w_sem,
    ag_send,
    ag_recv,
    rs_send,
    rs_recv,
    xg_send,
    xg_recv,
    xr_send,
    xr_recv,
):
    nz, nx, cap, rows, cols, pad = cfg
    half = nz // 2
    sub = rows // PARTS
    ep = lax.axis_index("ep")
    x = lax.axis_index("tp")
    z, c = ep // CORES, ep % CORES

    def wrap(v, n):
        return lax.rem(v + 2 * n, n)

    z_to = (
        {"ep": wrap(z + 1, nz) * CORES + c},
        {"ep": wrap(z - 1, nz) * CORES + c},
    )
    sib = z * CORES + 1 - c
    near, far_side = pl.ds(0, 2 * cap), pl.ds(2 * cap, 2 * cap)

    moves = [(r, own) for r in range(nx) for own in (True, False) if r or not own]
    moves.sort(key=lambda m: -min(m[0], nx - m[0]))
    peers = [
        {"tp": wrap(x + r, nx)} if own else {"tp": wrap(x + r, nx), "ep": sib} for r, own in moves
    ]

    def reach(d):
        return half - jnp.where(c == d, 0, 1)

    def hops(d, j):
        if j == PARTS:
            return reach(d)
        return reach(d) - (sub * j) // (CORES * cap)

    def remote(src, dst, ssem, rsem, dev):
        return pltpu.make_async_remote_copy(
            src_ref=src, dst_ref=dst, send_sem=ssem, recv_sem=rsem,
            device_id=dev, device_id_type=MESH,
        )

    def ag_copy(d, h, j):
        ssem = ag_send.at[d, lax.rem(h, 2), j]
        if j == PARTS:
            return remote(agm.at[d, h], agm.at[d, h + 1], ssem, ag_recv.at[d, h + 1, j], z_to[d])
        win = pl.ds(j * sub, sub)
        return remote(
            ag.at[d, h, win], ag.at[d, h + 1, win], ssem, ag_recv.at[d, h + 1, j], z_to[d]
        )

    def rs_copy(d, h, j):
        win = pl.ds(j * sub, sub)
        par = lax.rem(h, 2)
        return remote(
            rsend.at[d, par, win], rs.at[d, h - 1, win],
            rs_send.at[d, par, j], rs_recv.at[d, h - 1, j], z_to[1 - d],
        )

    def live(base, core, last):
        if last:
            return pl.ds(pl.multiple_of(base + core * cap, cap), cap)
        return pl.ds(base, 2 * cap)

    def xg_copy(h, n, last):
        own = moves[n][1]
        src = grow.at[x, h, live(0, c, last)] if own else stg.at[h, live(0, c, last)]
        dst = grow.at[x, h, live(0 if own else 2 * cap, c, last)]
        return remote(src, dst, xg_send.at[h, n], xg_recv.at[h, n], peers[n])

    def xr_copy(h, n, last):
        r, own = moves[n]
        core = c if own else 1 - c
        src = part.at[h, wrap(x + r, nx), live(0 if own else 2 * cap, core, last)]
        dst = inbox.at[h, n, live(0, core, last)]
        return remote(src, dst, xr_send.at[h, n], xr_recv.at[h, n], peers[n])

    def for_peers(copy, h, act):
        @pl.when(h == half)
        def _():
            for n in range(len(peers)):
                act(copy(h, n, True))

        @pl.when(h != half)
        def _():
            for n in range(len(peers)):
                act(copy(h, n, False))

    def start(copy):
        copy.start()

    def arrived(copy):
        copy.wait_recv()

    def left(copy):
        copy.wait_send()

    barrier = pltpu.get_barrier_semaphore()
    for dev in (*z_to, *peers):
        pl.semaphore_signal(barrier, inc=1, device_id=dev, device_id_type=MESH)

    loads = [
        pltpu.make_async_copy(src, dst, w_sem.at[3 + k])
        for k, (src, dst) in enumerate(
            ((ids_hbm, ids_in), (gate_hbm, gate_in), (tok_hbm, tok), (gain_hbm, gain))
        )
    ]
    for copy in loads:
        copy.start()
    weights = [
        pltpu.make_async_copy(src.at[0], dst, w_sem.at[k])
        for k, (src, dst) in enumerate(((wg_hbm, wg), (wu_hbm, wu), (wd_hbm, wd)))
    ]
    for copy in weights:
        copy.start()

    idle = jnp.zeros((cap, cols), BF16)
    for r in range(nx):
        grow[r, half, live(0, 1 - c, True)] = idle
        grow[r, half, live(2 * cap, c, True)] = idle
    for n in range(len(peers)):
        inbox[half, n, live(0, 1 - c, True)] = idle
    for d in range(2):
        for j in range(PARTS + 1):
            low = half - 1 - (0 if j == PARTS else (sub * j) // (CORES * cap))
            for h in range(max(low, 0), half + 1):
                if j < PARTS:
                    @pl.when(h >= hops(d, j))
                    def _():
                        rs[d, h, pl.ds(j * sub, sub)] = jnp.zeros((sub, cols), BF16)
                if h >= 1:
                    @pl.when(h > hops(d, j))
                    def _():
                        if j < PARTS:
                            ag[d, h, pl.ds(j * sub, sub)] = jnp.zeros((sub, cols), BF16)
                        else:
                            agm[d, h] = jnp.full((8, pad), -1.0, BF16)

    meta_in[...] = jnp.full((8, pad), -1.0, F32)
    loads[0].wait()
    loads[1].wait()
    meta_in[0:4, 0:rows] = ids_in[...].astype(F32)
    meta_in[4:8, 0:rows] = gate_in[...]
    meta = meta_in[...]
    ids = meta[0:4].astype(jnp.int32)
    ahead = lax.shift_right_arithmetic(ids, 1) - z
    ahead = jnp.where(ahead < 0, ahead + nz, ahead)
    behind = jnp.where(ahead == 0, 0, nz - ahead)
    lane = lax.broadcasted_iota(jnp.int32, (pad, pad), 1)
    line = lax.broadcasted_iota(jnp.int32, (pad, pad), 0)
    orders = []
    for d, dist in enumerate((ahead, behind)):
        far = jnp.max(jnp.where(dist <= reach(d), dist, 0), axis=0, keepdims=True)
        far = jnp.where(lane[0:1] < rows, far, -1).astype(F32)
        by_lane = jnp.broadcast_to(far, (pad, pad))
        by_line = by_lane.T
        first = (by_line > by_lane) | ((by_line == by_lane) & (line < lane))
        rank_lane = jnp.sum(jnp.where(first, 1.0, 0.0), axis=0, keepdims=True)
        later = (by_lane > by_line) | ((by_lane == by_line) & (lane < line))
        rank_line = jnp.sum(jnp.where(later, 1.0, 0.0), axis=1, keepdims=True)
        order = jnp.where(rank_lane == line.astype(F32), 1.0, 0.0).astype(BF16)
        back_to = jnp.where(rank_line == lane.astype(F32), 1.0, 0.0).astype(BF16)
        orders.append(order[:rows, :rows])
        agm[d, 0] = jnp.dot(
            meta.astype(BF16), back_to, preferred_element_type=F32
        ).astype(BF16)
        back[d] = back_to

    loads[2].wait()
    loads[3].wait()
    widened = tok[...].astype(F32)
    scale = lax.rsqrt(jnp.mean(widened * widened, axis=-1, keepdims=True) + epsilon)
    mine = pl.ds(pl.multiple_of(x * cols, cols), cols)
    own_cols = tok[:, mine].astype(F32) * scale
    own_cols = (own_cols * gain[:, mine]).astype(BF16)
    for d in range(2):
        ag[d, 0] = jnp.dot(orders[d], own_cols, preferred_element_type=F32).astype(BF16)

    for copy in weights:
        copy.wait()

    pl.semaphore_wait(barrier, 2 + len(peers))

    sub_line = lax.broadcasted_iota(jnp.int32, (2 * cap, pad), 0)
    own_slot = jnp.where(sub_line < cap, sub_line, sub_line - cap).astype(F32)

    def select(d, h):
        valid = h <= reach(d)
        if d == 1:
            valid = valid & (h >= 1)
        expert = jnp.where(sub_line < cap, ep, sib)
        expert = jnp.where(valid, expert, -7).astype(F32)
        meta = agm[d, h].astype(F32)
        named = jnp.zeros((2 * cap, pad), F32)
        weight = jnp.zeros((2 * cap, pad), F32)
        for k in range(4):
            same = jnp.where(meta[k : k + 1] == expert, 1.0, 0.0)
            named = named + same
            weight = weight + same * meta[k + 4 : k + 5]
        before = jnp.where(
            lax.broadcasted_iota(jnp.int32, (pad, pad), 0)
            < lax.broadcasted_iota(jnp.int32, (pad, pad), 1),
            1.0, 0.0,
        ).astype(BF16)
        slot = jnp.dot(named.astype(BF16), before, preferred_element_type=F32)
        pick = jnp.where(slot == own_slot, named, 0.0)
        spread = (pick * weight).astype(BF16)
        eye = jnp.where(
            lax.broadcasted_iota(jnp.int32, (rows, pad), 0)
            == lax.broadcasted_iota(jnp.int32, (rows, pad), 1),
            1.0, 0.0,
        ).astype(BF16)
        cbuf[d, h] = lax.dot_general(
            eye, spread, (((1,), (1,)), ((), ())), preferred_element_type=F32
        ).astype(BF16)
        got = jnp.dot(
            pick.astype(BF16)[:, :rows], ag[d, h], preferred_element_type=F32
        ).astype(BF16)
        grow[x, h, pl.ds(d * cap, cap)] = got[:cap]
        stg[h, pl.ds(d * cap, cap)] = got[cap:]

    def expert(h):
        for_peers(xg_copy, h, arrived)
        gate = jnp.zeros((4 * cap, wg.shape[1]), F32)
        up = jnp.zeros((4 * cap, wg.shape[1]), F32)
        for k in range(nx):
            block = grow[k, h]
            gate = gate + jnp.dot(
                block, wg[pl.ds(k * cols, cols)], preferred_element_type=F32
            )
            up = up + jnp.dot(block, wu[pl.ds(k * cols, cols)], preferred_element_type=F32)
        gated = jnp.minimum(gate, clamp_limit)
        linear = jnp.clip(up, -clamp_limit, clamp_limit)
        active = (gated * jax.nn.sigmoid(swish_alpha * gated) * (linear + 1.0)).astype(BF16)
        for k in range(nx):
            part[h, k] = jnp.dot(
                active, wd[:, pl.ds(k * cols, cols)], preferred_element_type=F32
            ).astype(BF16)

    def dispatch(i, _):
        for j in (PARTS, *range(PARTS)):
            for d in range(2):
                @pl.when((i >= 1) & (i <= hops(d, j)))
                def _():
                    ag_copy(d, i - 1, j).wait_recv()

                @pl.when(i < hops(d, j))
                def _():
                    @pl.when(i >= 2)
                    def _():
                        ag_copy(d, i - 2, j).wait_send()

                    ag_copy(d, i, j).start()

        for d in range(2):
            @pl.when(i <= reach(d))
            def _():
                select(d, i)

        for_peers(xg_copy, i, start)
        @pl.when(i >= 2)
        def _():
            expert(i - 2)

        return 0

    lax.fori_loop(0, half + 1, dispatch, 0)

    def spread_out(h):
        for_peers(xr_copy, h, arrived)
        y_own = part[h, x, near].astype(F32)
        y_sib = jnp.zeros_like(y_own)
        for n, (_, own) in enumerate(moves):
            if own:
                y_own = y_own + inbox[h, n].astype(F32)
            else:
                y_sib = y_sib + inbox[h, n].astype(F32)
        y_own, y_sib = y_own.astype(BF16), y_sib.astype(BF16)
        for d in range(2):
            both = jnp.concatenate(
                [y_own[d * cap : (d + 1) * cap], y_sib[d * cap : (d + 1) * cap]], axis=0
            )
            gains[d] = jnp.dot(cbuf[d, h], both, preferred_element_type=F32)

    def blend(d, h, j):
        win = pl.ds(j * sub, sub)
        return rs[d, h, win].astype(F32) + gains[d, win]

    def gather_back(i, _):
        @pl.when(i >= 2)
        def _():
            h = half - i + 2

            @pl.when(h + 2 <= half)
            def _():
                for_peers(xr_copy, h + 2, left)

            spread_out(h)
            for j in range(PARTS):
                for d in range(2):
                    @pl.when(h + 1 <= hops(d, j))
                    def _():
                        rs_copy(d, h + 1, j).wait_recv()

                    @pl.when(h + 2 <= hops(d, j))
                    def _():
                        rs_copy(d, h + 2, j).wait_send()

                    @pl.when(h <= hops(d, j))
                    def _():
                        rsend[d, lax.rem(h, 2), pl.ds(j * sub, sub)] = blend(d, h, j).astype(BF16)
                        rs_copy(d, h, j).start()

        @pl.when(i <= half)
        def _():
            h = half - i
            @pl.when(i < 2)
            def _():
                expert(h)

            for_peers(xr_copy, h, start)
            for_peers(xg_copy, h, left)

        return 0

    lax.fori_loop(0, half + 2, gather_back, 0)

    for h in range(min(3, half + 1)):
        for_peers(xr_copy, h, left)
    for d in range(2):
        for j in range(PARTS + 1):
            for k in (1, 2):
                @pl.when(hops(d, j) >= k)
                def _():
                    ag_copy(d, hops(d, j) - k, j).wait_send()

    spread_out(0)
    total = jnp.zeros((rows, cols), F32)
    for d in range(2):
        for j in range(PARTS):
            @pl.when(1 <= hops(d, j))
            def _():
                rs_copy(d, 1, j).wait_recv()
        held = jnp.concatenate(
            [blend(d, 0, j).astype(BF16) for j in range(PARTS)], axis=0
        )
        total = total + jnp.dot(back[d, :rows, :rows], held, preferred_element_type=F32)
    out_ref[...] = total.astype(BF16)

    for d in range(2):
        for j in range(PARTS):
            for k in (1, 2):
                @pl.when(hops(d, j) >= k)
                def _():
                    rs_copy(d, k, j).wait_send()


def body(ep_count, tp_count, tokens, norm_gain, w_gate, w_up, w_down, expert_ids, gate_weights):
    rows, width = tokens.shape
    top = expert_ids.shape[1]
    experts = w_gate.shape[0] * ep_count
    cap = min(rows, rows * top * 4 // (3 * experts))
    cols = width // tp_count
    hidden = w_gate.shape[2]
    pad = -(-rows // 128) * 128
    steps = ep_count // CORES // 2 + 1
    vmem = pl.BlockSpec(memory_space=pltpu.VMEM)
    hbm = pl.BlockSpec(memory_space=pl.ANY)
    dma = pltpu.SemaphoreType.DMA
    block = (4 * cap, cols)
    return pl.pallas_call(
        functools.partial(kernel, (ep_count // CORES, tp_count, cap, rows, cols, pad)),
        out_shape=jax.ShapeDtypeStruct((rows, cols), BF16),
        in_specs=[hbm] * 7,
        out_specs=vmem,
        scratch_shapes=[
            pltpu.VMEM((2, steps, rows, cols), BF16),
            pltpu.VMEM((2, steps, 8, pad), BF16),
            pltpu.VMEM((2, steps, rows, cols), BF16),
            pltpu.VMEM((2, 2, rows, cols), BF16),
            pltpu.VMEM((tp_count, steps, *block), BF16),
            pltpu.VMEM((steps, 2 * cap, cols), BF16),
            pltpu.VMEM((steps, tp_count, *block), BF16),
            pltpu.VMEM((steps, 2 * tp_count - 1, 2 * cap, cols), BF16),
            pltpu.VMEM((2, steps, rows, 2 * cap), BF16),
            pltpu.VMEM((2, rows, cols), F32),
            pltpu.VMEM((2, pad, pad), BF16),
            pltpu.VMEM((rows, width), BF16),
            pltpu.VMEM((1, width), F32),
            pltpu.VMEM((top, rows), jnp.int32),
            pltpu.VMEM((top, rows), F32),
            pltpu.VMEM((8, pad), F32),
            pltpu.VMEM((width, hidden), BF16),
            pltpu.VMEM((width, hidden), BF16),
            pltpu.VMEM((hidden, width), BF16),
            dma((7,)),
            dma((2, 2, PARTS + 1)),
            dma((2, steps, PARTS + 1)),
            dma((2, 2, PARTS)),
            dma((2, steps, PARTS)),
            dma((steps, 2 * tp_count - 1)),
            dma((steps, 2 * tp_count - 1)),
            dma((steps, 2 * tp_count - 1)),
            dma((steps, 2 * tp_count - 1)),
        ],
        compiler_params=pltpu.CompilerParams(
            collective_id=0, has_side_effects=True, vmem_limit_bytes=60 * 1024 * 1024
        ),
    )(tokens, norm_gain.reshape(1, width), expert_ids.T, gate_weights.T, w_gate, w_up, w_down)


def solution(mesh):
    return jax.shard_map(
        functools.partial(body, mesh.shape["ep"], mesh.shape["tp"]),
        mesh=mesh,
        in_specs=(
            P(("grp", "ep"), None),
            P(),
            P("ep", None, "tp"),
            P("ep", None, "tp"),
            P("ep", "tp", None),
            P(("grp", "ep"), None),
            P(("grp", "ep"), None),
        ),
        out_specs=P(("grp", "ep"), "tp"),
        check_vma=False,
    )
```

```python
import functools

import jax
import jax.numpy as jnp
from jax import lax
from jax.experimental import pallas as pl
from jax.experimental.pallas import tpu as pltpu
from jax.sharding import PartitionSpec as P

MESH = pl.DeviceIdType.MESH
BF16 = jnp.bfloat16
F32 = jnp.float32

epsilon = 1e-06
clamp_limit = 7.0
swish_alpha = 1.702

CORES = 2
AHEAD = 4
PARTS = 6


def kernel(
    cfg,
    tok_hbm,
    gain_hbm,
    ids_hbm,
    gate_hbm,
    wg_hbm,
    wu_hbm,
    wd_hbm,
    out_ref,
    ag,
    agm,
    rs,
    rsend,
    grow,
    stg,
    part,
    inbox,
    cbuf,
    gains,
    back,
    tok,
    gain,
    ids_in,
    gate_in,
    meta_in,
    wg,
    wu,
    wd,
    w_sem,
    ag_send,
    ag_recv,
    rs_send,
    rs_recv,
    xg_send,
    xg_recv,
    xr_send,
    xr_recv,
):
    nz, nx, cap, rows, cols, pad = cfg
    half = nz // 2
    sub = rows // PARTS
    ep = lax.axis_index("ep")
    x = lax.axis_index("tp")
    z, c = ep // CORES, ep % CORES

    def wrap(v, n):
        return lax.rem(v + 2 * n, n)

    z_to = (
        {"ep": wrap(z + 1, nz) * CORES + c},
        {"ep": wrap(z - 1, nz) * CORES + c},
    )
    sib = z * CORES + 1 - c
    near, far_side = pl.ds(0, 2 * cap), pl.ds(2 * cap, 2 * cap)

    moves = [(r, own) for r in range(nx) for own in (True, False) if r or not own]
    moves.sort(key=lambda m: -min(m[0], nx - m[0]))
    peers = [
        {"tp": wrap(x + r, nx)} if own else {"tp": wrap(x + r, nx), "ep": sib} for r, own in moves
    ]

    def reach(d):
        return half - jnp.where(c == d, 0, 1)

    def hops(d, j):
        if j == PARTS:
            return reach(d)
        return reach(d) - (sub * j) // (CORES * cap)

    def remote(src, dst, ssem, rsem, dev):
        return pltpu.make_async_remote_copy(
            src_ref=src, dst_ref=dst, send_sem=ssem, recv_sem=rsem,
            device_id=dev, device_id_type=MESH,
        )

    def ag_copy(d, h, j):
        ssem = ag_send.at[d, lax.rem(h, 2), j]
        if j == PARTS:
            return remote(agm.at[d, h], agm.at[d, h + 1], ssem, ag_recv.at[d, h + 1, j], z_to[d])
        win = pl.ds(j * sub, sub)
        return remote(
            ag.at[d, h, win], ag.at[d, h + 1, win], ssem, ag_recv.at[d, h + 1, j], z_to[d]
        )

    def rs_copy(d, h, j):
        win = pl.ds(j * sub, sub)
        par = lax.rem(h, 2)
        return remote(
            rsend.at[d, par, win], rs.at[d, h - 1, win],
            rs_send.at[d, par, j], rs_recv.at[d, h - 1, j], z_to[1 - d],
        )

    def live(base, core, last):
        if last:
            return pl.ds(pl.multiple_of(base + core * cap, cap), cap)
        return pl.ds(base, 2 * cap)

    def xg_copy(h, n, last):
        own = moves[n][1]
        src = grow.at[x, h, live(0, c, last)] if own else stg.at[h, live(0, c, last)]
        dst = grow.at[x, h, live(0 if own else 2 * cap, c, last)]
        return remote(src, dst, xg_send.at[h, n], xg_recv.at[h, n], peers[n])

    def xr_copy(h, n, last):
        r, own = moves[n]
        core = c if own else 1 - c
        src = part.at[h, wrap(x + r, nx), live(0 if own else 2 * cap, core, last)]
        dst = inbox.at[h, n, live(0, core, last)]
        return remote(src, dst, xr_send.at[h, n], xr_recv.at[h, n], peers[n])

    def for_peers(copy, h, act):
        @pl.when(h == half)
        def _():
            for n in range(len(peers)):
                act(copy(h, n, True))

        @pl.when(h != half)
        def _():
            for n in range(len(peers)):
                act(copy(h, n, False))

    def start(copy):
        copy.start()

    def arrived(copy):
        copy.wait_recv()

    def left(copy):
        copy.wait_send()

    barrier = pltpu.get_barrier_semaphore()
    for dev in (*z_to, *peers):
        pl.semaphore_signal(barrier, inc=1, device_id=dev, device_id_type=MESH)

    loads = [
        pltpu.make_async_copy(src, dst, w_sem.at[3 + k])
        for k, (src, dst) in enumerate(
            ((ids_hbm, ids_in), (gate_hbm, gate_in), (tok_hbm, tok), (gain_hbm, gain))
        )
    ]
    for copy in loads:
        copy.start()
    weights = [
        pltpu.make_async_copy(src.at[0], dst, w_sem.at[k])
        for k, (src, dst) in enumerate(((wg_hbm, wg), (wu_hbm, wu), (wd_hbm, wd)))
    ]
    for copy in weights:
        copy.start()

    idle = jnp.zeros((cap, cols), BF16)
    for r in range(nx):
        grow[r, half, live(0, 1 - c, True)] = idle
        grow[r, half, live(2 * cap, c, True)] = idle
    for n in range(len(peers)):
        inbox[half, n, live(0, 1 - c, True)] = idle
    for d in range(2):
        for j in range(PARTS + 1):
            low = half - 1 - (0 if j == PARTS else (sub * j) // (CORES * cap))
            for h in range(max(low, 0), half + 1):
                if j < PARTS:
                    @pl.when(h >= hops(d, j))
                    def _():
                        rs[d, h, pl.ds(j * sub, sub)] = jnp.zeros((sub, cols), BF16)
                if h >= 1:
                    @pl.when(h > hops(d, j))
                    def _():
                        if j < PARTS:
                            ag[d, h, pl.ds(j * sub, sub)] = jnp.zeros((sub, cols), BF16)
                        else:
                            agm[d, h] = jnp.full((8, pad), -1.0, BF16)

    meta_in[...] = jnp.full((8, pad), -1.0, F32)
    loads[0].wait()
    loads[1].wait()
    meta_in[0:4, 0:rows] = ids_in[...].astype(F32)
    meta_in[4:8, 0:rows] = gate_in[...]
    meta = meta_in[...]
    ids = meta[0:4].astype(jnp.int32)
    ahead = lax.shift_right_arithmetic(ids, 1) - z
    ahead = jnp.where(ahead < 0, ahead + nz, ahead)
    behind = jnp.where(ahead == 0, 0, nz - ahead)
    lane = lax.broadcasted_iota(jnp.int32, (pad, pad), 1)
    line = lax.broadcasted_iota(jnp.int32, (pad, pad), 0)
    orders = []
    for d, dist in enumerate((ahead, behind)):
        far = jnp.max(jnp.where(dist <= reach(d), dist, 0), axis=0, keepdims=True)
        far = jnp.where(lane[0:1] < rows, far, -1).astype(F32)
        by_lane = jnp.broadcast_to(far, (pad, pad))
        by_line = by_lane.T
        first = (by_line > by_lane) | ((by_line == by_lane) & (line < lane))
        rank_lane = jnp.sum(jnp.where(first, 1.0, 0.0), axis=0, keepdims=True)
        later = (by_lane > by_line) | ((by_lane == by_line) & (lane < line))
        rank_line = jnp.sum(jnp.where(later, 1.0, 0.0), axis=1, keepdims=True)
        order = jnp.where(rank_lane == line.astype(F32), 1.0, 0.0).astype(BF16)
        back_to = jnp.where(rank_line == lane.astype(F32), 1.0, 0.0).astype(BF16)
        orders.append(order[:rows, :rows])
        agm[d, 0] = jnp.dot(
            meta.astype(BF16), back_to, preferred_element_type=F32
        ).astype(BF16)
        back[d] = back_to

    loads[2].wait()
    loads[3].wait()
    widened = tok[...].astype(F32)
    scale = lax.rsqrt(jnp.mean(widened * widened, axis=-1, keepdims=True) + epsilon)
    mine = pl.ds(pl.multiple_of(x * cols, cols), cols)
    own_cols = tok[:, mine].astype(F32) * scale
    own_cols = (own_cols * gain[:, mine]).astype(BF16)
    for d in range(2):
        ag[d, 0] = jnp.dot(orders[d], own_cols, preferred_element_type=F32).astype(BF16)

    for copy in weights:
        copy.wait()

    pl.semaphore_wait(barrier, 2 + len(peers))

    sub_line = lax.broadcasted_iota(jnp.int32, (2 * cap, pad), 0)
    own_slot = jnp.where(sub_line < cap, sub_line, sub_line - cap).astype(F32)

    def select(d, h):
        valid = h <= reach(d)
        if d == 1:
            valid = valid & (h >= 1)
        expert = jnp.where(sub_line < cap, ep, sib)
        expert = jnp.where(valid, expert, -7).astype(F32)
        meta = agm[d, h].astype(F32)
        named = jnp.zeros((2 * cap, pad), F32)
        weight = jnp.zeros((2 * cap, pad), F32)
        for k in range(4):
            same = jnp.where(meta[k : k + 1] == expert, 1.0, 0.0)
            named = named + same
            weight = weight + same * meta[k + 4 : k + 5]
        before = jnp.where(
            lax.broadcasted_iota(jnp.int32, (pad, pad), 0)
            < lax.broadcasted_iota(jnp.int32, (pad, pad), 1),
            1.0, 0.0,
        ).astype(BF16)
        slot = jnp.dot(named.astype(BF16), before, preferred_element_type=F32)
        pick = jnp.where(slot == own_slot, named, 0.0)
        spread = (pick * weight).astype(BF16)
        eye = jnp.where(
            lax.broadcasted_iota(jnp.int32, (rows, pad), 0)
            == lax.broadcasted_iota(jnp.int32, (rows, pad), 1),
            1.0, 0.0,
        ).astype(BF16)
        cbuf[d, h] = lax.dot_general(
            eye, spread, (((1,), (1,)), ((), ())), preferred_element_type=F32
        ).astype(BF16)
        got = jnp.dot(
            pick.astype(BF16)[:, :rows], ag[d, h], preferred_element_type=F32
        ).astype(BF16)
        grow[x, h, pl.ds(d * cap, cap)] = got[:cap]
        stg[h, pl.ds(d * cap, cap)] = got[cap:]

    def expert(h):
        for_peers(xg_copy, h, arrived)
        gate = jnp.zeros((4 * cap, wg.shape[1]), F32)
        up = jnp.zeros((4 * cap, wg.shape[1]), F32)
        for k in range(nx):
            block = grow[k, h]
            gate = gate + jnp.dot(
                block, wg[pl.ds(k * cols, cols)], preferred_element_type=F32
            )
            up = up + jnp.dot(block, wu[pl.ds(k * cols, cols)], preferred_element_type=F32)
        gated = jnp.minimum(gate, clamp_limit)
        linear = jnp.clip(up, -clamp_limit, clamp_limit)
        active = (gated * jax.nn.sigmoid(swish_alpha * gated) * (linear + 1.0)).astype(BF16)
        for k in range(nx):
            part[h, k] = jnp.dot(
                active, wd[:, pl.ds(k * cols, cols)], preferred_element_type=F32
            ).astype(BF16)

    def dispatch(i, _):
        for j in (PARTS, *range(PARTS)):
            for d in range(2):
                @pl.when((i >= 1) & (i <= hops(d, j)))
                def _():
                    ag_copy(d, i - 1, j).wait_recv()

                @pl.when(i < hops(d, j))
                def _():
                    @pl.when(i >= 2)
                    def _():
                        ag_copy(d, i - 2, j).wait_send()

                    ag_copy(d, i, j).start()

        for d in range(2):
            @pl.when(i <= reach(d))
            def _():
                select(d, i)

        for_peers(xg_copy, i, start)
        @pl.when(i >= 2)
        def _():
            expert(i - 2)

        return 0

    lax.fori_loop(0, half + 1, dispatch, 0)

    def last_experts(k, _):
        expert(half - 1 + k)
        return 0

    lax.fori_loop(0, 2, last_experts, 0)

    def spread_out(h):
        for_peers(xr_copy, h, arrived)
        y_own = part[h, x, near].astype(F32)
        y_sib = jnp.zeros_like(y_own)
        for n, (_, own) in enumerate(moves):
            if own:
                y_own = y_own + inbox[h, n].astype(F32)
            else:
                y_sib = y_sib + inbox[h, n].astype(F32)
        y_own, y_sib = y_own.astype(BF16), y_sib.astype(BF16)
        for d in range(2):
            both = jnp.concatenate(
                [y_own[d * cap : (d + 1) * cap], y_sib[d * cap : (d + 1) * cap]], axis=0
            )
            gains[d] = jnp.dot(cbuf[d, h], both, preferred_element_type=F32)

    def blend(d, h, j):
        win = pl.ds(j * sub, sub)
        return rs[d, h, win].astype(F32) + gains[d, win]

    def gather_back(i, _):
        @pl.when(i <= half)
        def _():
            h = half - i
            for_peers(xr_copy, h, start)
            for_peers(xg_copy, h, left)

        @pl.when(i >= AHEAD)
        def _():
            h = half - i + AHEAD

            @pl.when(h + 2 <= half)
            def _():
                for_peers(xr_copy, h + 2, left)

            spread_out(h)
            for j in range(PARTS):
                for d in range(2):
                    @pl.when(h + 1 <= hops(d, j))
                    def _():
                        rs_copy(d, h + 1, j).wait_recv()

                    @pl.when(h + 2 <= hops(d, j))
                    def _():
                        rs_copy(d, h + 2, j).wait_send()

                    @pl.when(h <= hops(d, j))
                    def _():
                        rsend[d, lax.rem(h, 2), pl.ds(j * sub, sub)] = blend(d, h, j).astype(BF16)
                        rs_copy(d, h, j).start()

        return 0

    lax.fori_loop(0, half + AHEAD, gather_back, 0)

    for h in range(min(3, half + 1)):
        for_peers(xr_copy, h, left)
    for d in range(2):
        for j in range(PARTS + 1):
            for k in (1, 2):
                @pl.when(hops(d, j) >= k)
                def _():
                    ag_copy(d, hops(d, j) - k, j).wait_send()

    spread_out(0)
    total = jnp.zeros((rows, cols), F32)
    for d in range(2):
        for j in range(PARTS):
            @pl.when(1 <= hops(d, j))
            def _():
                rs_copy(d, 1, j).wait_recv()
        held = jnp.concatenate(
            [blend(d, 0, j).astype(BF16) for j in range(PARTS)], axis=0
        )
        total = total + jnp.dot(back[d, :rows, :rows], held, preferred_element_type=F32)
    out_ref[...] = total.astype(BF16)

    for d in range(2):
        for j in range(PARTS):
            for k in (1, 2):
                @pl.when(hops(d, j) >= k)
                def _():
                    rs_copy(d, k, j).wait_send()


def body(ep_count, tp_count, tokens, norm_gain, w_gate, w_up, w_down, expert_ids, gate_weights):
    rows, width = tokens.shape
    top = expert_ids.shape[1]
    experts = w_gate.shape[0] * ep_count
    cap = min(rows, rows * top * 4 // (3 * experts))
    cols = width // tp_count
    hidden = w_gate.shape[2]
    pad = -(-rows // 128) * 128
    steps = ep_count // CORES // 2 + 1
    vmem = pl.BlockSpec(memory_space=pltpu.VMEM)
    hbm = pl.BlockSpec(memory_space=pl.ANY)
    dma = pltpu.SemaphoreType.DMA
    block = (4 * cap, cols)
    return pl.pallas_call(
        functools.partial(kernel, (ep_count // CORES, tp_count, cap, rows, cols, pad)),
        out_shape=jax.ShapeDtypeStruct((rows, cols), BF16),
        in_specs=[hbm] * 7,
        out_specs=vmem,
        scratch_shapes=[
            pltpu.VMEM((2, steps, rows, cols), BF16),
            pltpu.VMEM((2, steps, 8, pad), BF16),
            pltpu.VMEM((2, steps, rows, cols), BF16),
            pltpu.VMEM((2, 2, rows, cols), BF16),
            pltpu.VMEM((tp_count, steps, *block), BF16),
            pltpu.VMEM((steps, 2 * cap, cols), BF16),
            pltpu.VMEM((steps, tp_count, *block), BF16),
            pltpu.VMEM((steps, 2 * tp_count - 1, 2 * cap, cols), BF16),
            pltpu.VMEM((2, steps, rows, 2 * cap), BF16),
            pltpu.VMEM((2, rows, cols), F32),
            pltpu.VMEM((2, pad, pad), BF16),
            pltpu.VMEM((rows, width), BF16),
            pltpu.VMEM((1, width), F32),
            pltpu.VMEM((top, rows), jnp.int32),
            pltpu.VMEM((top, rows), F32),
            pltpu.VMEM((8, pad), F32),
            pltpu.VMEM((width, hidden), BF16),
            pltpu.VMEM((width, hidden), BF16),
            pltpu.VMEM((hidden, width), BF16),
            dma((7,)),
            dma((2, 2, PARTS + 1)),
            dma((2, steps, PARTS + 1)),
            dma((2, 2, PARTS)),
            dma((2, steps, PARTS)),
            dma((steps, 2 * tp_count - 1)),
            dma((steps, 2 * tp_count - 1)),
            dma((steps, 2 * tp_count - 1)),
            dma((steps, 2 * tp_count - 1)),
        ],
        compiler_params=pltpu.CompilerParams(
            collective_id=0, has_side_effects=True, vmem_limit_bytes=60 * 1024 * 1024
        ),
    )(tokens, norm_gain.reshape(1, width), expert_ids.T, gate_weights.T, w_gate, w_up, w_down)


def solution(mesh):
    return jax.shard_map(
        functools.partial(body, mesh.shape["ep"], mesh.shape["tp"]),
        mesh=mesh,
        in_specs=(
            P(("grp", "ep"), None),
            P(),
            P("ep", None, "tp"),
            P("ep", None, "tp"),
            P("ep", "tp", None),
            P(("grp", "ep"), None),
            P(("grp", "ep"), None),
        ),
        out_specs=P(("grp", "ep"), "tp"),
        check_vma=False,
    )
```

```python
import functools

import jax
import jax.numpy as jnp
from jax import lax
from jax.experimental import pallas as pl
from jax.experimental.pallas import tpu as pltpu
from jax.sharding import PartitionSpec as P

MESH = pl.DeviceIdType.MESH
BF16 = jnp.bfloat16
F32 = jnp.float32

epsilon = 1e-06
clamp_limit = 7.0
swish_alpha = 1.702

CORES = 2
AHEAD = 4
PARTS = 6


def kernel(
    cfg,
    tok_hbm,
    gain_hbm,
    ids_hbm,
    gate_hbm,
    wg_hbm,
    wu_hbm,
    wd_hbm,
    out_ref,
    ag,
    agm,
    rs,
    rsend,
    grow,
    stg,
    part,
    inbox,
    cbuf,
    gains,
    back,
    tok,
    gain,
    ids_in,
    gate_in,
    meta_in,
    wg,
    wu,
    wd,
    w_sem,
    ag_send,
    ag_recv,
    rs_send,
    rs_recv,
    xg_send,
    xg_recv,
    xr_send,
    xr_recv,
):
    nz, nx, cap, rows, cols, pad = cfg
    half = nz // 2
    sub = rows // PARTS
    ep = lax.axis_index("ep")
    x = lax.axis_index("tp")
    z, c = ep // CORES, ep % CORES

    def wrap(v, n):
        return lax.rem(v + 2 * n, n)

    z_to = (
        {"ep": wrap(z + 1, nz) * CORES + c},
        {"ep": wrap(z - 1, nz) * CORES + c},
    )
    sib = z * CORES + 1 - c
    near, far_side = pl.ds(0, 2 * cap), pl.ds(2 * cap, 2 * cap)

    moves = [(r, own) for r in range(nx) for own in (True, False) if r or not own]
    moves.sort(key=lambda m: -min(m[0], nx - m[0]))
    peers = [
        {"tp": wrap(x + r, nx)} if own else {"tp": wrap(x + r, nx), "ep": sib} for r, own in moves
    ]

    def reach(d):
        return half - jnp.where(c == d, 0, 1)

    def hops(d, j):
        if j == PARTS:
            return reach(d)
        return reach(d) - (sub * j) // (CORES * cap)

    def remote(src, dst, ssem, rsem, dev):
        return pltpu.make_async_remote_copy(
            src_ref=src, dst_ref=dst, send_sem=ssem, recv_sem=rsem,
            device_id=dev, device_id_type=MESH,
        )

    def ag_copy(d, h, j):
        ssem = ag_send.at[d, lax.rem(h, 2), j]
        if j == PARTS:
            return remote(agm.at[d, h], agm.at[d, h + 1], ssem, ag_recv.at[d, h + 1, j], z_to[d])
        win = pl.ds(j * sub, sub)
        return remote(
            ag.at[d, h, win], ag.at[d, h + 1, win], ssem, ag_recv.at[d, h + 1, j], z_to[d]
        )

    def rs_copy(d, h, j):
        win = pl.ds(j * sub, sub)
        par = lax.rem(h, 2)
        return remote(
            rsend.at[d, par, win], rs.at[d, h - 1, win],
            rs_send.at[d, par, j], rs_recv.at[d, h - 1, j], z_to[1 - d],
        )

    def live(base, core, last):
        if last:
            return pl.ds(pl.multiple_of(base + core * cap, cap), cap)
        return pl.ds(base, 2 * cap)

    def xg_copy(h, n, last):
        own = moves[n][1]
        src = grow.at[x, h, live(0, c, last)] if own else stg.at[h, live(0, c, last)]
        dst = grow.at[x, h, live(0 if own else 2 * cap, c, last)]
        return remote(src, dst, xg_send.at[h, n], xg_recv.at[h, n], peers[n])

    def xr_copy(h, n, last):
        r, own = moves[n]
        core = c if own else 1 - c
        src = part.at[h, wrap(x + r, nx), live(0 if own else 2 * cap, core, last)]
        dst = inbox.at[h, n, live(0, core, last)]
        return remote(src, dst, xr_send.at[h, n], xr_recv.at[h, n], peers[n])

    def for_peers(copy, h, act):
        @pl.when(h == half)
        def _():
            for n in range(len(peers)):
                act(copy(h, n, True))

        @pl.when(h != half)
        def _():
            for n in range(len(peers)):
                act(copy(h, n, False))

    def start(copy):
        copy.start()

    def arrived(copy):
        copy.wait_recv()

    def left(copy):
        copy.wait_send()

    barrier = pltpu.get_barrier_semaphore()
    for dev in (*z_to, *peers):
        pl.semaphore_signal(barrier, inc=1, device_id=dev, device_id_type=MESH)

    loads = [
        pltpu.make_async_copy(src, dst, w_sem.at[3 + k])
        for k, (src, dst) in enumerate(
            ((ids_hbm, ids_in), (gate_hbm, gate_in), (tok_hbm, tok), (gain_hbm, gain))
        )
    ]
    for copy in loads:
        copy.start()
    weights = [
        pltpu.make_async_copy(src.at[0], dst, w_sem.at[k])
        for k, (src, dst) in enumerate(((wg_hbm, wg), (wu_hbm, wu), (wd_hbm, wd)))
    ]
    for copy in weights:
        copy.start()

    idle = jnp.zeros((cap, cols), BF16)
    for r in range(nx):
        grow[r, half, live(0, 1 - c, True)] = idle
        grow[r, half, live(2 * cap, c, True)] = idle
    for n in range(len(peers)):
        inbox[half, n, live(0, 1 - c, True)] = idle
    for d in range(2):
        for j in range(PARTS + 1):
            low = half - 1 - (0 if j == PARTS else (sub * j) // (CORES * cap))
            for h in range(max(low, 0), half + 1):
                if j < PARTS:
                    @pl.when(h >= hops(d, j))
                    def _():
                        rs[d, h, pl.ds(j * sub, sub)] = jnp.zeros((sub, cols), BF16)
                if h >= 1:
                    @pl.when(h > hops(d, j))
                    def _():
                        if j < PARTS:
                            ag[d, h, pl.ds(j * sub, sub)] = jnp.zeros((sub, cols), BF16)
                        else:
                            agm[d, h] = jnp.full((8, pad), -1.0, BF16)

    meta_in[...] = jnp.full((8, pad), -1.0, F32)
    loads[0].wait()
    loads[1].wait()
    meta_in[0:4, 0:rows] = ids_in[...].astype(F32)
    meta_in[4:8, 0:rows] = gate_in[...]
    meta = meta_in[...]
    ids = meta[0:4].astype(jnp.int32)
    ahead = lax.shift_right_arithmetic(ids, 1) - z
    ahead = jnp.where(ahead < 0, ahead + nz, ahead)
    behind = jnp.where(ahead == 0, 0, nz - ahead)
    lane = lax.broadcasted_iota(jnp.int32, (pad, pad), 1)
    line = lax.broadcasted_iota(jnp.int32, (pad, pad), 0)
    orders = []
    for d, dist in enumerate((ahead, behind)):
        far = jnp.max(jnp.where(dist <= reach(d), dist, 0), axis=0, keepdims=True)
        far = jnp.where(lane[0:1] < rows, far, -1).astype(F32)
        by_lane = jnp.broadcast_to(far, (pad, pad))
        by_line = by_lane.T
        first = (by_line > by_lane) | ((by_line == by_lane) & (line < lane))
        rank_lane = jnp.sum(jnp.where(first, 1.0, 0.0), axis=0, keepdims=True)
        later = (by_lane > by_line) | ((by_lane == by_line) & (lane < line))
        rank_line = jnp.sum(jnp.where(later, 1.0, 0.0), axis=1, keepdims=True)
        order = jnp.where(rank_lane == line.astype(F32), 1.0, 0.0).astype(BF16)
        back_to = jnp.where(rank_line == lane.astype(F32), 1.0, 0.0).astype(BF16)
        orders.append(order[:rows, :rows])
        agm[d, 0] = jnp.dot(
            meta.astype(BF16), back_to, preferred_element_type=F32
        ).astype(BF16)
        back[d] = back_to

    loads[2].wait()
    loads[3].wait()
    widened = tok[...].astype(F32)
    scale = lax.rsqrt(jnp.mean(widened * widened, axis=-1, keepdims=True) + epsilon)
    mine = pl.ds(pl.multiple_of(x * cols, cols), cols)
    own_cols = tok[:, mine].astype(F32) * scale
    own_cols = (own_cols * gain[:, mine]).astype(BF16)
    for d in range(2):
        ag[d, 0] = jnp.dot(orders[d], own_cols, preferred_element_type=F32).astype(BF16)

    for copy in weights:
        copy.wait()

    pl.semaphore_wait(barrier, 2 + len(peers))

    sub_line = lax.broadcasted_iota(jnp.int32, (2 * cap, pad), 0)
    own_slot = jnp.where(sub_line < cap, sub_line, sub_line - cap).astype(F32)

    def select(d, h):
        valid = h <= reach(d)
        if d == 1:
            valid = valid & (h >= 1)
        expert = jnp.where(sub_line < cap, ep, sib)
        expert = jnp.where(valid, expert, -7).astype(F32)
        meta = agm[d, h].astype(F32)
        named = jnp.zeros((2 * cap, pad), F32)
        weight = jnp.zeros((2 * cap, pad), F32)
        for k in range(4):
            same = jnp.where(meta[k : k + 1] == expert, 1.0, 0.0)
            named = named + same
            weight = weight + same * meta[k + 4 : k + 5]
        before = jnp.where(
            lax.broadcasted_iota(jnp.int32, (pad, pad), 0)
            < lax.broadcasted_iota(jnp.int32, (pad, pad), 1),
            1.0, 0.0,
        ).astype(BF16)
        slot = jnp.dot(named.astype(BF16), before, preferred_element_type=F32)
        pick = jnp.where(slot == own_slot, named, 0.0)
        spread = (pick * weight).astype(BF16)
        eye = jnp.where(
            lax.broadcasted_iota(jnp.int32, (rows, pad), 0)
            == lax.broadcasted_iota(jnp.int32, (rows, pad), 1),
            1.0, 0.0,
        ).astype(BF16)
        cbuf[d, h] = lax.dot_general(
            eye, spread, (((1,), (1,)), ((), ())), preferred_element_type=F32
        ).astype(BF16)
        got = jnp.dot(
            pick.astype(BF16)[:, :rows], ag[d, h], preferred_element_type=F32
        ).astype(BF16)
        grow[x, h, pl.ds(d * cap, cap)] = got[:cap]
        stg[h, pl.ds(d * cap, cap)] = got[cap:]

    def expert(h):
        for_peers(xg_copy, h, arrived)
        gate = jnp.zeros((4 * cap, wg.shape[1]), F32)
        up = jnp.zeros((4 * cap, wg.shape[1]), F32)
        for k in range(nx):
            block = grow[k, h]
            gate = gate + jnp.dot(
                block, wg[pl.ds(k * cols, cols)], preferred_element_type=F32
            )
            up = up + jnp.dot(block, wu[pl.ds(k * cols, cols)], preferred_element_type=F32)
        gated = jnp.minimum(gate, clamp_limit)
        linear = jnp.clip(up, -clamp_limit, clamp_limit)
        active = (gated * jax.nn.sigmoid(swish_alpha * gated) * (linear + 1.0)).astype(BF16)
        for k in range(nx):
            part[h, k] = jnp.dot(
                active, wd[:, pl.ds(k * cols, cols)], preferred_element_type=F32
            ).astype(BF16)

    def dispatch(i, _):
        for j in (PARTS, *range(PARTS)):
            for d in range(2):
                @pl.when((i >= 1) & (i <= hops(d, j)))
                def _():
                    ag_copy(d, i - 1, j).wait_recv()

                @pl.when(i < hops(d, j))
                def _():
                    @pl.when(i >= 2)
                    def _():
                        ag_copy(d, i - 2, j).wait_send()

                    ag_copy(d, i, j).start()

        for d in range(2):
            @pl.when(i <= reach(d))
            def _():
                select(d, i)

        for_peers(xg_copy, i, start)
        @pl.when(i >= 3)
        def _():
            expert(i - 3)

        return 0

    lax.fori_loop(0, half + 1, dispatch, 0)

    def last_experts(k, _):
        expert(half - 2 + k)
        return 0

    lax.fori_loop(0, 3, last_experts, 0)

    def spread_out(h):
        for_peers(xr_copy, h, arrived)
        y_own = part[h, x, near].astype(F32)
        y_sib = jnp.zeros_like(y_own)
        for n, (_, own) in enumerate(moves):
            if own:
                y_own = y_own + inbox[h, n].astype(F32)
            else:
                y_sib = y_sib + inbox[h, n].astype(F32)
        y_own, y_sib = y_own.astype(BF16), y_sib.astype(BF16)
        for d in range(2):
            both = jnp.concatenate(
                [y_own[d * cap : (d + 1) * cap], y_sib[d * cap : (d + 1) * cap]], axis=0
            )
            gains[d] = jnp.dot(cbuf[d, h], both, preferred_element_type=F32)

    def blend(d, h, j):
        win = pl.ds(j * sub, sub)
        return rs[d, h, win].astype(F32) + gains[d, win]

    def gather_back(i, _):
        @pl.when(i <= half)
        def _():
            h = half - i
            for_peers(xr_copy, h, start)
            for_peers(xg_copy, h, left)

        @pl.when(i >= AHEAD)
        def _():
            h = half - i + AHEAD

            @pl.when(h + 2 <= half)
            def _():
                for_peers(xr_copy, h + 2, left)

            spread_out(h)
            for j in range(PARTS):
                for d in range(2):
                    @pl.when(h + 1 <= hops(d, j))
                    def _():
                        rs_copy(d, h + 1, j).wait_recv()

                    @pl.when(h + 2 <= hops(d, j))
                    def _():
                        rs_copy(d, h + 2, j).wait_send()

                    @pl.when(h <= hops(d, j))
                    def _():
                        rsend[d, lax.rem(h, 2), pl.ds(j * sub, sub)] = blend(d, h, j).astype(BF16)
                        rs_copy(d, h, j).start()

        return 0

    lax.fori_loop(0, half + AHEAD, gather_back, 0)

    for h in range(min(3, half + 1)):
        for_peers(xr_copy, h, left)
    for d in range(2):
        for j in range(PARTS + 1):
            for k in (1, 2):
                @pl.when(hops(d, j) >= k)
                def _():
                    ag_copy(d, hops(d, j) - k, j).wait_send()

    spread_out(0)
    total = jnp.zeros((rows, cols), F32)
    for d in range(2):
        for j in range(PARTS):
            @pl.when(1 <= hops(d, j))
            def _():
                rs_copy(d, 1, j).wait_recv()
        held = jnp.concatenate(
            [blend(d, 0, j).astype(BF16) for j in range(PARTS)], axis=0
        )
        total = total + jnp.dot(back[d, :rows, :rows], held, preferred_element_type=F32)
    out_ref[...] = total.astype(BF16)

    for d in range(2):
        for j in range(PARTS):
            for k in (1, 2):
                @pl.when(hops(d, j) >= k)
                def _():
                    rs_copy(d, k, j).wait_send()


def body(ep_count, tp_count, tokens, norm_gain, w_gate, w_up, w_down, expert_ids, gate_weights):
    rows, width = tokens.shape
    top = expert_ids.shape[1]
    experts = w_gate.shape[0] * ep_count
    cap = min(rows, rows * top * 4 // (3 * experts))
    cols = width // tp_count
    hidden = w_gate.shape[2]
    pad = -(-rows // 128) * 128
    steps = ep_count // CORES // 2 + 1
    vmem = pl.BlockSpec(memory_space=pltpu.VMEM)
    hbm = pl.BlockSpec(memory_space=pl.ANY)
    dma = pltpu.SemaphoreType.DMA
    block = (4 * cap, cols)
    return pl.pallas_call(
        functools.partial(kernel, (ep_count // CORES, tp_count, cap, rows, cols, pad)),
        out_shape=jax.ShapeDtypeStruct((rows, cols), BF16),
        in_specs=[hbm] * 7,
        out_specs=vmem,
        scratch_shapes=[
            pltpu.VMEM((2, steps, rows, cols), BF16),
            pltpu.VMEM((2, steps, 8, pad), BF16),
            pltpu.VMEM((2, steps, rows, cols), BF16),
            pltpu.VMEM((2, 2, rows, cols), BF16),
            pltpu.VMEM((tp_count, steps, *block), BF16),
            pltpu.VMEM((steps, 2 * cap, cols), BF16),
            pltpu.VMEM((steps, tp_count, *block), BF16),
            pltpu.VMEM((steps, 2 * tp_count - 1, 2 * cap, cols), BF16),
            pltpu.VMEM((2, steps, rows, 2 * cap), BF16),
            pltpu.VMEM((2, rows, cols), F32),
            pltpu.VMEM((2, pad, pad), BF16),
            pltpu.VMEM((rows, width), BF16),
            pltpu.VMEM((1, width), F32),
            pltpu.VMEM((top, rows), jnp.int32),
            pltpu.VMEM((top, rows), F32),
            pltpu.VMEM((8, pad), F32),
            pltpu.VMEM((width, hidden), BF16),
            pltpu.VMEM((width, hidden), BF16),
            pltpu.VMEM((hidden, width), BF16),
            dma((7,)),
            dma((2, 2, PARTS + 1)),
            dma((2, steps, PARTS + 1)),
            dma((2, 2, PARTS)),
            dma((2, steps, PARTS)),
            dma((steps, 2 * tp_count - 1)),
            dma((steps, 2 * tp_count - 1)),
            dma((steps, 2 * tp_count - 1)),
            dma((steps, 2 * tp_count - 1)),
        ],
        compiler_params=pltpu.CompilerParams(
            collective_id=0, has_side_effects=True, vmem_limit_bytes=60 * 1024 * 1024
        ),
    )(tokens, norm_gain.reshape(1, width), expert_ids.T, gate_weights.T, w_gate, w_up, w_down)


def solution(mesh):
    return jax.shard_map(
        functools.partial(body, mesh.shape["ep"], mesh.shape["tp"]),
        mesh=mesh,
        in_specs=(
            P(("grp", "ep"), None),
            P(),
            P("ep", None, "tp"),
            P("ep", None, "tp"),
            P("ep", "tp", None),
            P(("grp", "ep"), None),
            P(("grp", "ep"), None),
        ),
        out_specs=P(("grp", "ep"), "tp"),
        check_vma=False,
    )
```

```python
import functools

import jax
import jax.numpy as jnp
from jax import lax
from jax.experimental import pallas as pl
from jax.experimental.pallas import tpu as pltpu
from jax.sharding import PartitionSpec as P

MESH = pl.DeviceIdType.MESH
BF16 = jnp.bfloat16
F32 = jnp.float32

epsilon = 1e-06
clamp_limit = 7.0
swish_alpha = 1.702

CORES = 2
AHEAD = 5
PARTS = 6


def kernel(
    cfg,
    tok_hbm,
    gain_hbm,
    ids_hbm,
    gate_hbm,
    wg_hbm,
    wu_hbm,
    wd_hbm,
    out_ref,
    ag,
    agm,
    rs,
    rsend,
    grow,
    stg,
    part,
    inbox,
    cbuf,
    gains,
    back,
    tok,
    gain,
    ids_in,
    gate_in,
    meta_in,
    wg,
    wu,
    wd,
    w_sem,
    ag_send,
    ag_recv,
    rs_send,
    rs_recv,
    xg_send,
    xg_recv,
    xr_send,
    xr_recv,
):
    nz, nx, cap, rows, cols, pad = cfg
    half = nz // 2
    sub = rows // PARTS
    ep = lax.axis_index("ep")
    x = lax.axis_index("tp")
    z, c = ep // CORES, ep % CORES

    def wrap(v, n):
        return lax.rem(v + 2 * n, n)

    z_to = (
        {"ep": wrap(z + 1, nz) * CORES + c},
        {"ep": wrap(z - 1, nz) * CORES + c},
    )
    sib = z * CORES + 1 - c
    near, far_side = pl.ds(0, 2 * cap), pl.ds(2 * cap, 2 * cap)

    moves = [(r, own) for r in range(nx) for own in (True, False) if r or not own]
    moves.sort(key=lambda m: -min(m[0], nx - m[0]))
    peers = [
        {"tp": wrap(x + r, nx)} if own else {"tp": wrap(x + r, nx), "ep": sib} for r, own in moves
    ]

    def reach(d):
        return half - jnp.where(c == d, 0, 1)

    def hops(d, j):
        if j == PARTS:
            return reach(d)
        return reach(d) - (sub * j) // (CORES * cap)

    def remote(src, dst, ssem, rsem, dev):
        return pltpu.make_async_remote_copy(
            src_ref=src, dst_ref=dst, send_sem=ssem, recv_sem=rsem,
            device_id=dev, device_id_type=MESH,
        )

    def ag_copy(d, h, j):
        ssem = ag_send.at[d, lax.rem(h, 2), j]
        if j == PARTS:
            return remote(agm.at[d, h], agm.at[d, h + 1], ssem, ag_recv.at[d, h + 1, j], z_to[d])
        win = pl.ds(j * sub, sub)
        return remote(
            ag.at[d, h, win], ag.at[d, h + 1, win], ssem, ag_recv.at[d, h + 1, j], z_to[d]
        )

    def rs_copy(d, h, j):
        win = pl.ds(j * sub, sub)
        par = lax.rem(h, 2)
        return remote(
            rsend.at[d, par, win], rs.at[d, h - 1, win],
            rs_send.at[d, par, j], rs_recv.at[d, h - 1, j], z_to[1 - d],
        )

    def live(base, core, last):
        if last:
            return pl.ds(pl.multiple_of(base + core * cap, cap), cap)
        return pl.ds(base, 2 * cap)

    def xg_copy(h, n, last):
        own = moves[n][1]
        src = grow.at[x, h, live(0, c, last)] if own else stg.at[h, live(0, c, last)]
        dst = grow.at[x, h, live(0 if own else 2 * cap, c, last)]
        return remote(src, dst, xg_send.at[h, n], xg_recv.at[h, n], peers[n])

    def xr_copy(h, n, last):
        r, own = moves[n]
        core = c if own else 1 - c
        src = part.at[h, wrap(x + r, nx), live(0 if own else 2 * cap, core, last)]
        dst = inbox.at[h, n, live(0, core, last)]
        return remote(src, dst, xr_send.at[h, n], xr_recv.at[h, n], peers[n])

    def for_peers(copy, h, act):
        @pl.when(h == half)
        def _():
            for n in range(len(peers)):
                act(copy(h, n, True))

        @pl.when(h != half)
        def _():
            for n in range(len(peers)):
                act(copy(h, n, False))

    def start(copy):
        copy.start()

    def arrived(copy):
        copy.wait_recv()

    def left(copy):
        copy.wait_send()

    barrier = pltpu.get_barrier_semaphore()
    for dev in (*z_to, *peers):
        pl.semaphore_signal(barrier, inc=1, device_id=dev, device_id_type=MESH)

    loads = [
        pltpu.make_async_copy(src, dst, w_sem.at[3 + k])
        for k, (src, dst) in enumerate(
            ((ids_hbm, ids_in), (gate_hbm, gate_in), (tok_hbm, tok), (gain_hbm, gain))
        )
    ]
    for copy in loads:
        copy.start()
    weights = [
        pltpu.make_async_copy(src.at[0], dst, w_sem.at[k])
        for k, (src, dst) in enumerate(((wg_hbm, wg), (wu_hbm, wu), (wd_hbm, wd)))
    ]
    for copy in weights:
        copy.start()

    idle = jnp.zeros((cap, cols), BF16)
    for r in range(nx):
        grow[r, half, live(0, 1 - c, True)] = idle
        grow[r, half, live(2 * cap, c, True)] = idle
    for n in range(len(peers)):
        inbox[half, n, live(0, 1 - c, True)] = idle
    for d in range(2):
        for j in range(PARTS + 1):
            low = half - 1 - (0 if j == PARTS else (sub * j) // (CORES * cap))
            for h in range(max(low, 0), half + 1):
                if j < PARTS:
                    @pl.when(h >= hops(d, j))
                    def _():
                        rs[d, h, pl.ds(j * sub, sub)] = jnp.zeros((sub, cols), BF16)
                if h >= 1:
                    @pl.when(h > hops(d, j))
                    def _():
                        if j < PARTS:
                            ag[d, h, pl.ds(j * sub, sub)] = jnp.zeros((sub, cols), BF16)
                        else:
                            agm[d, h] = jnp.full((8, pad), -1.0, BF16)

    meta_in[...] = jnp.full((8, pad), -1.0, F32)
    loads[0].wait()
    loads[1].wait()
    meta_in[0:4, 0:rows] = ids_in[...].astype(F32)
    meta_in[4:8, 0:rows] = gate_in[...]
    meta = meta_in[...]
    ids = meta[0:4].astype(jnp.int32)
    ahead = lax.shift_right_arithmetic(ids, 1) - z
    ahead = jnp.where(ahead < 0, ahead + nz, ahead)
    behind = jnp.where(ahead == 0, 0, nz - ahead)
    lane = lax.broadcasted_iota(jnp.int32, (pad, pad), 1)
    line = lax.broadcasted_iota(jnp.int32, (pad, pad), 0)
    orders = []
    for d, dist in enumerate((ahead, behind)):
        far = jnp.max(jnp.where(dist <= reach(d), dist, 0), axis=0, keepdims=True)
        far = jnp.where(lane[0:1] < rows, far, -1).astype(F32)
        by_lane = jnp.broadcast_to(far, (pad, pad))
        by_line = by_lane.T
        first = (by_line > by_lane) | ((by_line == by_lane) & (line < lane))
        rank_lane = jnp.sum(jnp.where(first, 1.0, 0.0), axis=0, keepdims=True)
        later = (by_lane > by_line) | ((by_lane == by_line) & (lane < line))
        rank_line = jnp.sum(jnp.where(later, 1.0, 0.0), axis=1, keepdims=True)
        order = jnp.where(rank_lane == line.astype(F32), 1.0, 0.0).astype(BF16)
        back_to = jnp.where(rank_line == lane.astype(F32), 1.0, 0.0).astype(BF16)
        orders.append(order[:rows, :rows])
        agm[d, 0] = jnp.dot(
            meta.astype(BF16), back_to, preferred_element_type=F32
        ).astype(BF16)
        back[d] = back_to

    loads[2].wait()
    loads[3].wait()
    widened = tok[...].astype(F32)
    scale = lax.rsqrt(jnp.mean(widened * widened, axis=-1, keepdims=True) + epsilon)
    mine = pl.ds(pl.multiple_of(x * cols, cols), cols)
    own_cols = tok[:, mine].astype(F32) * scale
    own_cols = (own_cols * gain[:, mine]).astype(BF16)
    for d in range(2):
        ag[d, 0] = jnp.dot(orders[d], own_cols, preferred_element_type=F32).astype(BF16)

    for copy in weights:
        copy.wait()

    pl.semaphore_wait(barrier, 2 + len(peers))

    sub_line = lax.broadcasted_iota(jnp.int32, (2 * cap, pad), 0)
    own_slot = jnp.where(sub_line < cap, sub_line, sub_line - cap).astype(F32)

    def select(d, h):
        valid = h <= reach(d)
        if d == 1:
            valid = valid & (h >= 1)
        expert = jnp.where(sub_line < cap, ep, sib)
        expert = jnp.where(valid, expert, -7).astype(F32)
        meta = agm[d, h].astype(F32)
        named = jnp.zeros((2 * cap, pad), F32)
        weight = jnp.zeros((2 * cap, pad), F32)
        for k in range(4):
            same = jnp.where(meta[k : k + 1] == expert, 1.0, 0.0)
            named = named + same
            weight = weight + same * meta[k + 4 : k + 5]
        before = jnp.where(
            lax.broadcasted_iota(jnp.int32, (pad, pad), 0)
            < lax.broadcasted_iota(jnp.int32, (pad, pad), 1),
            1.0, 0.0,
        ).astype(BF16)
        slot = jnp.dot(named.astype(BF16), before, preferred_element_type=F32)
        pick = jnp.where(slot == own_slot, named, 0.0)
        spread = (pick * weight).astype(BF16)
        eye = jnp.where(
            lax.broadcasted_iota(jnp.int32, (rows, pad), 0)
            == lax.broadcasted_iota(jnp.int32, (rows, pad), 1),
            1.0, 0.0,
        ).astype(BF16)
        cbuf[d, h] = lax.dot_general(
            eye, spread, (((1,), (1,)), ((), ())), preferred_element_type=F32
        ).astype(BF16)
        got = jnp.dot(
            pick.astype(BF16)[:, :rows], ag[d, h], preferred_element_type=F32
        ).astype(BF16)
        grow[x, h, pl.ds(d * cap, cap)] = got[:cap]
        stg[h, pl.ds(d * cap, cap)] = got[cap:]

    def expert(h):
        for_peers(xg_copy, h, arrived)
        gate = jnp.zeros((4 * cap, wg.shape[1]), F32)
        up = jnp.zeros((4 * cap, wg.shape[1]), F32)
        for k in range(nx):
            block = grow[k, h]
            gate = gate + jnp.dot(
                block, wg[pl.ds(k * cols, cols)], preferred_element_type=F32
            )
            up = up + jnp.dot(block, wu[pl.ds(k * cols, cols)], preferred_element_type=F32)
        gated = jnp.minimum(gate, clamp_limit)
        linear = jnp.clip(up, -clamp_limit, clamp_limit)
        active = (gated * jax.nn.sigmoid(swish_alpha * gated) * (linear + 1.0)).astype(BF16)
        for k in range(nx):
            part[h, k] = jnp.dot(
                active, wd[:, pl.ds(k * cols, cols)], preferred_element_type=F32
            ).astype(BF16)

    def dispatch(i, _):
        for j in (PARTS, *range(PARTS)):
            for d in range(2):
                @pl.when((i >= 1) & (i <= hops(d, j)))
                def _():
                    ag_copy(d, i - 1, j).wait_recv()

                @pl.when(i < hops(d, j))
                def _():
                    @pl.when(i >= 2)
                    def _():
                        ag_copy(d, i - 2, j).wait_send()

                    ag_copy(d, i, j).start()

        for d in range(2):
            @pl.when(i <= reach(d))
            def _():
                select(d, i)

        for_peers(xg_copy, i, start)
        @pl.when(i >= 3)
        def _():
            expert(i - 3)

        return 0

    lax.fori_loop(0, half + 1, dispatch, 0)

    def last_experts(k, _):
        expert(half - 2 + k)
        return 0

    lax.fori_loop(0, 3, last_experts, 0)

    def spread_out(h):
        for_peers(xr_copy, h, arrived)
        y_own = part[h, x, near].astype(F32)
        y_sib = jnp.zeros_like(y_own)
        for n, (_, own) in enumerate(moves):
            if own:
                y_own = y_own + inbox[h, n].astype(F32)
            else:
                y_sib = y_sib + inbox[h, n].astype(F32)
        y_own, y_sib = y_own.astype(BF16), y_sib.astype(BF16)
        for d in range(2):
            both = jnp.concatenate(
                [y_own[d * cap : (d + 1) * cap], y_sib[d * cap : (d + 1) * cap]], axis=0
            )
            gains[d] = jnp.dot(cbuf[d, h], both, preferred_element_type=F32)

    def blend(d, h, j):
        win = pl.ds(j * sub, sub)
        return rs[d, h, win].astype(F32) + gains[d, win]

    def gather_back(i, _):
        @pl.when(i <= half)
        def _():
            h = half - i
            for_peers(xr_copy, h, start)
            for_peers(xg_copy, h, left)

        @pl.when(i >= AHEAD)
        def _():
            h = half - i + AHEAD

            @pl.when(h + 2 <= half)
            def _():
                for_peers(xr_copy, h + 2, left)

            spread_out(h)
            for j in range(PARTS):
                for d in range(2):
                    @pl.when(h + 1 <= hops(d, j))
                    def _():
                        rs_copy(d, h + 1, j).wait_recv()

                    @pl.when(h + 2 <= hops(d, j))
                    def _():
                        rs_copy(d, h + 2, j).wait_send()

                    @pl.when(h <= hops(d, j))
                    def _():
                        rsend[d, lax.rem(h, 2), pl.ds(j * sub, sub)] = blend(d, h, j).astype(BF16)
                        rs_copy(d, h, j).start()

        return 0

    lax.fori_loop(0, half + AHEAD, gather_back, 0)

    for h in range(min(3, half + 1)):
        for_peers(xr_copy, h, left)
    for d in range(2):
        for j in range(PARTS + 1):
            for k in (1, 2):
                @pl.when(hops(d, j) >= k)
                def _():
                    ag_copy(d, hops(d, j) - k, j).wait_send()

    spread_out(0)
    total = jnp.zeros((rows, cols), F32)
    for d in range(2):
        for j in range(PARTS):
            @pl.when(1 <= hops(d, j))
            def _():
                rs_copy(d, 1, j).wait_recv()
        held = jnp.concatenate(
            [blend(d, 0, j).astype(BF16) for j in range(PARTS)], axis=0
        )
        total = total + jnp.dot(back[d, :rows, :rows], held, preferred_element_type=F32)
    out_ref[...] = total.astype(BF16)

    for d in range(2):
        for j in range(PARTS):
            for k in (1, 2):
                @pl.when(hops(d, j) >= k)
                def _():
                    rs_copy(d, k, j).wait_send()


def body(ep_count, tp_count, tokens, norm_gain, w_gate, w_up, w_down, expert_ids, gate_weights):
    rows, width = tokens.shape
    top = expert_ids.shape[1]
    experts = w_gate.shape[0] * ep_count
    cap = min(rows, rows * top * 4 // (3 * experts))
    cols = width // tp_count
    hidden = w_gate.shape[2]
    pad = -(-rows // 128) * 128
    steps = ep_count // CORES // 2 + 1
    vmem = pl.BlockSpec(memory_space=pltpu.VMEM)
    hbm = pl.BlockSpec(memory_space=pl.ANY)
    dma = pltpu.SemaphoreType.DMA
    block = (4 * cap, cols)
    return pl.pallas_call(
        functools.partial(kernel, (ep_count // CORES, tp_count, cap, rows, cols, pad)),
        out_shape=jax.ShapeDtypeStruct((rows, cols), BF16),
        in_specs=[hbm] * 7,
        out_specs=vmem,
        scratch_shapes=[
            pltpu.VMEM((2, steps, rows, cols), BF16),
            pltpu.VMEM((2, steps, 8, pad), BF16),
            pltpu.VMEM((2, steps, rows, cols), BF16),
            pltpu.VMEM((2, 2, rows, cols), BF16),
            pltpu.VMEM((tp_count, steps, *block), BF16),
            pltpu.VMEM((steps, 2 * cap, cols), BF16),
            pltpu.VMEM((steps, tp_count, *block), BF16),
            pltpu.VMEM((steps, 2 * tp_count - 1, 2 * cap, cols), BF16),
            pltpu.VMEM((2, steps, rows, 2 * cap), BF16),
            pltpu.VMEM((2, rows, cols), F32),
            pltpu.VMEM((2, pad, pad), BF16),
            pltpu.VMEM((rows, width), BF16),
            pltpu.VMEM((1, width), F32),
            pltpu.VMEM((top, rows), jnp.int32),
            pltpu.VMEM((top, rows), F32),
            pltpu.VMEM((8, pad), F32),
            pltpu.VMEM((width, hidden), BF16),
            pltpu.VMEM((width, hidden), BF16),
            pltpu.VMEM((hidden, width), BF16),
            dma((7,)),
            dma((2, 2, PARTS + 1)),
            dma((2, steps, PARTS + 1)),
            dma((2, 2, PARTS)),
            dma((2, steps, PARTS)),
            dma((steps, 2 * tp_count - 1)),
            dma((steps, 2 * tp_count - 1)),
            dma((steps, 2 * tp_count - 1)),
            dma((steps, 2 * tp_count - 1)),
        ],
        compiler_params=pltpu.CompilerParams(
            collective_id=0, has_side_effects=True, vmem_limit_bytes=60 * 1024 * 1024
        ),
    )(tokens, norm_gain.reshape(1, width), expert_ids.T, gate_weights.T, w_gate, w_up, w_down)


def solution(mesh):
    return jax.shard_map(
        functools.partial(body, mesh.shape["ep"], mesh.shape["tp"]),
        mesh=mesh,
        in_specs=(
            P(("grp", "ep"), None),
            P(),
            P("ep", None, "tp"),
            P("ep", None, "tp"),
            P("ep", "tp", None),
            P(("grp", "ep"), None),
            P(("grp", "ep"), None),
        ),
        out_specs=P(("grp", "ep"), "tp"),
        check_vma=False,
    )
```
